256 devices in a mesh: sp: 64 (over z, y, core), tp: 4 (over x).
Axes of the slice: x: 4, y: 4, z: 8, core: 2. Of those that a mesh axis runs over, the one named last changes fastest.
Arguments:
- stream: bfloat16 [24576, 2048], P(('sp', 'tp')), may hold values from -6 to 6
- query_projected: bfloat16 [24576, 1024], P('sp', 'tp'), may hold values from -6 to 6
- key_projected: bfloat16 [24576, 1024], P('sp', 'tp'), may hold values from -6 to 6
- value_projected: bfloat16 [24576, 1024], P('sp', 'tp'), may hold values from -6 to 6
- gate_projected: bfloat16 [24576, 1024], P('sp', 'tp'), may hold values from -6 to 6
- strength_logits: bfloat16 [8, 24576], P('tp', 'sp'), may hold values from -7 to 4
- decay_preactivation: bfloat16 [8, 24576], P('tp', 'sp'), may hold values from -9 to 9
- extra_log_decay: float32 [8, 24576], P('tp', 'sp'), may hold values from -0.7 to 0
- head_decay_rate: float32 [8], P('tp'), may hold values from 0 to 0.1
- head_norm_gain: float32 [128], replicated, may hold values from 0.1 to 1.9
- head_output_matrix: bfloat16 [1024, 2048], P('tp'), may hold values from -0.1875 to 0.1875
- feed_norm_gain: float32 [2048], replicated, may hold values from 0.1 to 1.9
- gate_matrix: bfloat16 [2048, 5632], P('sp', 'tp'), may hold values from -0.125 to 0.125
- up_matrix: bfloat16 [2048, 5632], P('sp', 'tp'), may hold values from -0.125 to 0.125
- down_matrix: bfloat16 [5632, 2048], P('tp', 'sp'), may hold values from -0.078125 to 0.078125
Outputs:
- result: bfloat16 [24576, 2048], P(('sp', 'tp'))
The draws below stay inside these ranges and needn't reach their ends.
All inputs are finite; a program needn't handle non-finite values.
Results may differ from the reference program's by a relative error of at most 0.015.
Values may be sent and summed in bfloat16 or wider, within the bound.
A program may use at most 128 MiB of HBM per device.

```python
import math
import jax
import jax.numpy as jnp
from jax import lax

D = 2048
HEADS = 8
HEAD = 128
FF = 5632
BLOCK = 64
TOK_DEV = 384
HK = 1024
TOKENS = 24576
N_TP = 4


def head_ranking(key):
    return jax.random.permutation(jax.random.fold_in(key, 101), HEADS)


def fast_heads(key):
    fast_count = HEADS // 2
    return head_ranking(key) < fast_count


def draw_head_decay_rate(key, part):
    is_fast = fast_heads(key)
    slow_rate = jnp.exp(jax.random.uniform(jax.random.fold_in(key, 102), (HEADS,), jnp.float32, math.log(0.01), math.log(0.3))) / TOKENS
    fast_rate = jnp.exp(jax.random.uniform(jax.random.fold_in(key, 103), (HEADS,), jnp.float32, math.log(0.03), math.log(0.1)))
    return jnp.where(is_fast, fast_rate, slow_rate).astype(jnp.float32)


def draw_strength_logits(key, part):
    is_fast = fast_heads(key)
    fast_part = jnp.clip(jax.random.normal(jax.random.fold_in(key, 401), (HEADS, TOKENS), jnp.float32), -4.0, 4.0)
    faint_part = jax.random.uniform(jax.random.fold_in(key, 402), (HEADS, TOKENS), jnp.float32, -7.0, -5.0)
    return jnp.where(is_fast[:, None], fast_part, faint_part).astype(jnp.bfloat16)


def draw_decay_preactivation(key, part):
    block_total = TOKENS // TOK_DEV
    noise = jnp.clip(jax.random.normal(jax.random.fold_in(key, 201), (HEADS, block_total, TOK_DEV), jnp.float32), -6.0, 6.0)
    offsets = jax.random.uniform(jax.random.fold_in(key, 202), (block_total,), jnp.float32, -1.5, 1.5)
    return (noise + offsets[None, :, None]).reshape(HEADS, TOKENS).astype(jnp.bfloat16)


def draw_extra_log_decay(key, part):
    places = jax.random.randint(jax.random.fold_in(key, 301), (3,), 0, TOKENS)
    levels = jax.random.uniform(jax.random.fold_in(key, 302), (HEADS, 3), jnp.float32, math.log(0.5), math.log(0.8))
    base = jnp.zeros((HEADS, TOKENS), jnp.float32)
    return base.at[:, places].set(levels).astype(jnp.float32)


def steps_of(stream_key, extent, pieces, low, largest):
    def one(dim, blocks):
        heights = jax.random.uniform(jax.random.fold_in(jax.random.fold_in(stream_key, 6), dim), (blocks,), jnp.float32, low / len(pieces), largest / len(pieces))
        return jnp.repeat(jnp.exp(heights), extent[dim] // blocks).reshape((-1,) + (1,) * (len(extent) - dim - 1))

    level = one(*pieces[0])
    for cut in pieces[1:]:
        level = level * one(*cut)
    return level


def bell_draw(own_key, extent, scale, reach, cuts=(), kind=jnp.bfloat16):
    loudness = steps_of(own_key, extent, cuts, -0.22, 0.18) if cuts else 1.0
    values = jax.random.normal(own_key, extent, jnp.float32) * scale * loudness
    return jnp.minimum(jnp.maximum(values, -reach), reach).astype(kind)


def setup_inputs(seed: int = 0) -> dict:
    seeds = jax.random.split(jax.random.key(seed), 16)
    stream = bell_draw(seeds[0], (TOKENS, D), 1.0, 6.0, ((0, 256),))
    query_projected = bell_draw(seeds[1], (TOKENS, HK), 1.0, 6.0, ((0, 64), (1, 4)))
    key_projected = bell_draw(seeds[2], (TOKENS, HK), 1.0, 6.0, ((0, 64), (1, 4)))
    value_projected = bell_draw(seeds[3], (TOKENS, HK), 1.0, 6.0, ((0, 64), (1, 4)))
    gate_projected = bell_draw(seeds[4], (TOKENS, HK), 1.0, 6.0, ((0, 64), (1, 4)))
    strength_logits = draw_strength_logits(jax.random.fold_in(seeds[15], 71), 0)
    decay_preactivation = draw_decay_preactivation(jax.random.fold_in(seeds[15], 71), 0)
    extra_log_decay = draw_extra_log_decay(jax.random.fold_in(seeds[15], 71), 0)
    head_decay_rate = draw_head_decay_rate(jax.random.fold_in(seeds[15], 71), 0)
    head_norm_gain = jnp.clip(1.0 + 0.18 * jax.random.normal(seeds[9], (HEAD,), jnp.float32), 0.1, 1.9)
    head_output_matrix = bell_draw(seeds[10], (HK, D), HK ** -0.5, 0.1875, ((0, 4),))
    feed_norm_gain = jnp.clip(1.0 + 0.18 * jax.random.normal(seeds[11], (D,), jnp.float32), 0.1, 1.9)
    gate_matrix = bell_draw(seeds[12], (D, FF), D ** -0.5, 0.125, ((0, 64), (1, 4)))
    up_matrix = bell_draw(seeds[13], (D, FF), D ** -0.5, 0.125, ((0, 64), (1, 4)))
    down_matrix = bell_draw(seeds[14], (FF, D), FF ** -0.5, 0.078125, ((0, 4), (1, 64)))
    return dict(stream=stream, query_projected=query_projected, key_projected=key_projected, value_projected=value_projected, gate_projected=gate_projected, strength_logits=strength_logits, decay_preactivation=decay_preactivation, extra_log_decay=extra_log_decay, head_decay_rate=head_decay_rate, head_norm_gain=head_norm_gain, head_output_matrix=head_output_matrix, feed_norm_gain=feed_norm_gain, gate_matrix=gate_matrix, up_matrix=up_matrix, down_matrix=down_matrix)


PRECISION_FULL = lax.Precision.HIGHEST
EPSILON = 1e-06

def unit_rows(tensor):
    return tensor * lax.rsqrt(lax.optimization_barrier(jnp.sum(tensor * tensor, axis=-1, keepdims=True)) + EPSILON)

def block_correction(unit_queries, unit_keys, complete_values, strength_logits, decay_preactivation, extra_log_decay, head_decay_rate):
    head_count, length, head_width = unit_queries.shape
    block_count = length // BLOCK

    def to_blocks(tensor):
        return tensor.reshape((head_count, block_count, BLOCK) + tensor.shape[2:])
    beta_gate = jax.nn.sigmoid(strength_logits.astype(jnp.float32))
    decay_logarithm = -head_decay_rate[:, None] * jax.nn.softplus(decay_preactivation.astype(jnp.float32)) + extra_log_decay
    query_block = to_blocks(unit_queries)
    key_block = to_blocks(unit_keys)
    value_block = to_blocks(complete_values)
    beta_block = to_blocks(beta_gate)
    cumulative = jnp.cumsum(to_blocks(decay_logarithm), axis=-1)
    causal = jnp.tril(jnp.ones((BLOCK, BLOCK), bool))
    strict = jnp.tril(jnp.ones((BLOCK, BLOCK), bool), -1)
    spread = cumulative[..., :, None] - cumulative[..., None, :]
    damping = jnp.where(causal, jnp.exp(jnp.where(causal, spread, 0.0)), 0.0)
    key_beta = key_block * beta_block[..., None]
    lower_part = jnp.einsum('hnid,hnjd->hnij', key_beta, key_block, precision=PRECISION_FULL) * jnp.where(strict, damping, 0.0)
    system = lower_part + jnp.eye(BLOCK, dtype=jnp.float32)
    right_side = jnp.concatenate([value_block * beta_block[..., None], key_beta * jnp.exp(cumulative)[..., None]], axis=-1)
    solved = lax.linalg.triangular_solve(system, right_side, left_side=True, lower=True, unit_diagonal=True)
    target_values = solved[..., :head_width]
    householder_weights = solved[..., head_width:]
    inner_scores = jnp.einsum('hnid,hnjd->hnij', query_block, key_block, precision=PRECISION_FULL) * damping
    decayed_queries = query_block * jnp.exp(cumulative)[..., None]
    closing_log_decay = cumulative[..., -1:]
    decayed_keys = key_block * jnp.exp(closing_log_decay - cumulative)[..., None]
    return (decayed_queries, decayed_keys, target_values, householder_weights, inner_scores, closing_log_decay)

def advance(running_state, items):
    decayed_queries, decayed_keys, target_values, householder_weights, inner_scores, closing_log_decay = items
    new_state = target_values - jnp.einsum('fdc,fcj->fdj', householder_weights, running_state, precision=PRECISION_FULL)
    layer_output = jnp.einsum('fdc,fcj->fdj', decayed_queries, running_state, precision=PRECISION_FULL)
    layer_output = layer_output + jnp.einsum('hij,hjv->hiv', inner_scores, new_state, precision=PRECISION_FULL)
    running_state = jnp.exp(closing_log_decay)[:, :, None] * running_state + jnp.einsum('xwp,xws->xps', decayed_keys, new_state, precision=PRECISION_FULL)
    return (running_state, layer_output)

def split_heads(tensor):
    return tensor.reshape(TOKENS, HEADS, HEAD).transpose(1, 0, 2).astype(jnp.float32)

def rms_scale(tensor):
    return tensor * lax.rsqrt(lax.optimization_barrier(jnp.mean(tensor * tensor, axis=-1, keepdims=True)) + EPSILON)

def reference(stream, query_projected, key_projected, value_projected, gate_projected, strength_logits, decay_preactivation, extra_log_decay, head_decay_rate, head_norm_gain, head_output_matrix, feed_norm_gain, gate_matrix, up_matrix, down_matrix):
    unit_queries = unit_rows(split_heads(query_projected)) * HEAD ** (-0.5)
    unit_keys = unit_rows(split_heads(key_projected))
    complete_values = split_heads(value_projected)
    score_terms = block_correction(unit_queries, unit_keys, complete_values, strength_logits, decay_preactivation, extra_log_decay, head_decay_rate)
    moved = tuple((jnp.moveaxis(tensor, 1, 0) for tensor in score_terms))
    initial = jnp.zeros((HEADS, HEAD, HEAD), jnp.float32)
    _, block_outputs = lax.scan(advance, initial, moved)
    attention_output = jnp.moveaxis(block_outputs, 0, 1).reshape(HEADS, TOKENS, HEAD)
    normed_heads = rms_scale(attention_output) * head_norm_gain
    gated = normed_heads.transpose(1, 0, 2).reshape(TOKENS, HK) * jax.nn.silu(gate_projected.astype(jnp.float32))
    mixed = gated.astype(jnp.bfloat16)
    group_width = HK // N_TP
    branch = jnp.zeros((TOKENS, D), jnp.float32)
    for group in range(N_TP):
        piece = jnp.dot(mixed[:, group * group_width:(group + 1) * group_width].astype(jnp.float32), head_output_matrix[group * group_width:(group + 1) * group_width].astype(jnp.float32), preferred_element_type=jnp.float32)
        branch = branch + piece.astype(jnp.bfloat16).astype(jnp.float32)
    residual = stream.astype(jnp.float32) + branch
    normed = (rms_scale(residual) * feed_norm_gain).astype(jnp.bfloat16)
    gate = jnp.dot(normed.astype(jnp.float32), gate_matrix.astype(jnp.float32), preferred_element_type=jnp.float32)
    up_value = jnp.dot(normed.astype(jnp.float32), up_matrix.astype(jnp.float32), preferred_element_type=jnp.float32)
    hidden = (jax.nn.silu(gate) * up_value).astype(jnp.bfloat16)
    unit_group = FF // N_TP
    ffn_total = jnp.zeros((TOKENS, D), jnp.float32)
    for group in range(N_TP):
        piece = jnp.dot(hidden[:, group * unit_group:(group + 1) * unit_group].astype(jnp.float32), down_matrix[group * unit_group:(group + 1) * unit_group].astype(jnp.float32), preferred_element_type=jnp.float32)
        ffn_total = ffn_total + piece.astype(jnp.bfloat16).astype(jnp.float32)
    return (residual + ffn_total).astype(jnp.bfloat16)
```

```python
import functools
import jax
import jax.numpy as jnp
from jax import lax
from jax.experimental import pallas as pl
from jax.experimental.pallas import tpu as pltpu
from jax.sharding import Mesh
from jax.sharding import PartitionSpec as P

HEAD = 128
CHUNK = 128
SP = ("sp_0", "sp_1", "sp_2")
SP_TP = ("sp_0", "sp_1", "sp_2", "tp")
EPSILON = 1e-06
F32 = jnp.float32
BF16 = jnp.bfloat16
HIGH = lax.Precision.HIGHEST
MESH = pl.DeviceIdType.MESH


def mm(a, b):
    return jnp.dot(a.astype(BF16), b.astype(BF16), preferred_element_type=F32)


def mm_nt(a, b):
    return lax.dot_general(a, b, (((1,), (1,)), ((), ())), preferred_element_type=F32)


def mm_tn(a, b):
    return lax.dot_general(
        a.astype(BF16), b.astype(BF16), (((0,), (0,)), ((), ())), preferred_element_type=F32
    )


def full(a, b):
    return jnp.dot(a, b, precision=HIGH, preferred_element_type=F32)


def full_nt(a, b):
    return lax.dot_general(
        a, b, (((1,), (1,)), ((), ())), precision=HIGH, preferred_element_type=F32
    )


def silu(x):
    return x / (1.0 + jnp.exp(-x))


def softplus(x):
    return jnp.maximum(x, 0.0) + jnp.log1p(jnp.exp(-jnp.abs(x)))


def unit_lower_inverses(lowers, row, col):
    inverses = []
    for lower in lowers:
        near = jnp.where((row >> 3) == (col >> 3), lower, 0.0)
        inverses.append((near, jnp.where(row == col, 1.0, 0.0) - near))
    squares = [full(d, d) for d, _ in inverses]
    inverses = [x + full(x, s) for (_, x), s in zip(inverses, squares)]
    squares = [full(s, s) for s in squares]
    inverses = [x + full(x, s) for x, s in zip(inverses, squares)]
    for level in (3, 4, 5, 6):
        between = ((row >> (level + 1)) == (col >> (level + 1))) & ((row >> level) != (col >> level))
        parts = [jnp.where(between, lower, 0.0) for lower in lowers]
        parts = [full(p, x) for p, x in zip(parts, inverses)]
        inverses = [x - full(x, p) for p, x in zip(parts, inverses)]
    return inverses


def local_part(
    q_ref, k_ref, v_ref, strength_ref, decay_ref, extra_ref, rate_ref, maps, from_state, from_values
):
    row = lax.broadcasted_iota(jnp.int32, (CHUNK, CHUNK), 0)
    col = lax.broadcasted_iota(jnp.int32, (CHUNK, CHUNK), 1)
    eye = jnp.where(row == col, 1.0, 0.0)
    lower_ones = jnp.where(row >= col, 1.0, 0.0)
    upper_ones = jnp.where(row <= col, 1.0, 0.0)
    padding = jnp.zeros((6, CHUNK), F32)

    def chunk(c, carry):
        span = pl.ds(pl.multiple_of(c * CHUNK, CHUNK), CHUNK)
        logs = -rate_ref[...] * softplus(decay_ref[:, span].astype(F32)) + extra_ref[:, span]
        beta = 1.0 / (1.0 + jnp.exp(-strength_ref[:, span].astype(F32)))
        logs = jnp.concatenate([logs, padding], axis=0)
        beta = jnp.concatenate([beta, padding], axis=0)
        sums_row = full(logs, upper_ones)
        sums_col = full_nt(lower_ones, logs)
        beta_col = full_nt(eye, beta)
        lowers, scores, rights, keys, queries, closings = [], [], [], [], [], []
        for h in range(2):
            cols = slice(h * HEAD, (h + 1) * HEAD)
            k = k_ref[span, cols]
            q = q_ref[span, cols]
            kf, qf, vf = k.astype(F32), q.astype(F32), v_ref[span, cols].astype(F32)
            squares = kf * kf
            k_col = lax.rsqrt(jnp.sum(squares, axis=1, keepdims=True) + EPSILON)
            k_row = lax.rsqrt(full_nt(jnp.ones((8, HEAD), F32), squares)[0:1] + EPSILON)
            q_col = lax.rsqrt(jnp.sum(qf * qf, axis=1, keepdims=True) + EPSILON) * HEAD ** (-0.5)
            s_col, s_row, b_col = sums_col[:, h : h + 1], sums_row[h : h + 1], beta_col[:, h : h + 1]
            closing = s_row[:, CHUNK - 1 :]
            damping = jnp.exp(jnp.minimum(s_col - s_row, 0.0)) * k_row
            lowers.append(jnp.where(row > col, mm_nt(k, k) * damping * (b_col * k_col), 0.0))
            scores.append(jnp.where(row >= col, mm_nt(q, k) * damping * q_col, 0.0))
            opening = jnp.exp(s_col)
            rights.append(
                jnp.concatenate([kf * (b_col * k_col * opening), vf * b_col], axis=1)
            )
            keys.append(kf * (k_col * jnp.exp(closing - s_col)))
            queries.append(qf * (q_col * opening))
            closings.append(jnp.exp(closing) - 1.0)
        inverses = unit_lower_inverses(lowers, row, col)
        solved = [r + mm(x - eye, r) for x, r in zip(inverses, rights)]
        for h in range(2):
            u = c * 2 + h
            change = mm_tn(keys[h], solved[h])
            maps[u, :, :HEAD] = closings[h] * eye - change[:, :HEAD]
            maps[u, :, HEAD:] = change[:, HEAD:]
            out = mm(scores[h], solved[h])
            from_state[u] = (queries[h] - out[:, :HEAD]).astype(BF16)
            from_values[u] = out[:, HEAD:]
        return carry

    lax.fori_loop(0, 3, chunk, 0)


def joined(earlier, later):
    return earlier + later + mm(later[:, :HEAD], earlier)


def carried(state, pair):
    return state + pair[:, HEAD:] + mm(pair[:, :HEAD], state)


def attention_kernel(
    q_ref,
    k_ref,
    v_ref,
    gate_ref,
    strength_ref,
    decay_ref,
    extra_ref,
    rate_ref,
    gain_ref,
    mixed_ref,
    maps,
    from_state,
    from_values,
    totals,
    pair,
    sib,
    chip,
    zin,
    zout,
    hin,
    hout,
    send_sem,
    recv_sem,
):
    z, y, c = lax.axis_index("sp_0"), lax.axis_index("sp_1"), lax.axis_index("sp_2")
    zin[...] = jnp.zeros_like(zin)
    barrier = pltpu.get_barrier_semaphore()
    peers = [{"sp_2": 1 - c}]
    peers += [{"sp_1": lax.rem(y + d, 4)} for d in (1, 2, 3)]
    peers += [{"sp_0": lax.rem(z + d, 8)} for d in (1, 7)]
    for peer in peers:
        pl.semaphore_signal(barrier, inc=1, device_id=peer, device_id_type=MESH)
    pl.semaphore_wait(barrier, len(peers))

    def copy(src, dst, slot, peer):
        return pltpu.make_async_remote_copy(
            src_ref=src,
            dst_ref=dst,
            send_sem=send_sem.at[slot],
            recv_sem=recv_sem.at[slot],
            device_id=peer,
            device_id_type=MESH,
        )

    local_part(
        q_ref, k_ref, v_ref, strength_ref, decay_ref, extra_ref, rate_ref, maps, from_state, from_values
    )
    for h in range(2):
        total = joined(joined(maps[h], maps[2 + h]), maps[4 + h])
        totals[h] = total
        pair[h] = total.astype(BF16)

    to_sib = copy(pair.at[1 - c], sib, 0, {"sp_2": 1 - c})
    to_sib.start()
    to_sib.wait()
    own, other = totals[c], sib[...].astype(F32)
    first = jnp.where(c == 0, own, other)
    second = jnp.where(c == 0, other, own)
    chip[y] = joined(first, second).astype(BF16)

    sends = []
    for d in (1, 2, 3):
        sends.append(copy(chip.at[y], chip.at[y], d, {"sp_1": lax.rem(y + d, 4)}))
        sends[-1].start()
    for d in (1, 2, 3):
        source = lax.rem(y + 4 - d, 4)
        copy(chip.at[source], chip.at[source], d, {"sp_1": lax.rem(y + d, 4)}).wait_recv()
    total = chip[0].astype(F32)
    before = jnp.where(y == 0, 0.0, total)
    for s in (1, 2, 3):
        total = joined(total, chip[s].astype(F32))
        if s < 3:
            before = jnp.where(y > s, total, before)
    for send in sends:
        send.wait_send()

    onward = copy(zout, zin, 4, {"sp_0": lax.rem(z + 1, 8)})

    @pl.when(z > 0)
    def _():
        onward.wait_recv()

    state = zin[...].astype(F32)

    @pl.when(z < 7)
    def _():
        zout[...] = carried(state, total).astype(BF16)
        onward.start()

    state = carried(state, before)
    later = carried(state, first)
    hout[...] = jnp.where(c == 0, later, state).astype(BF16)
    across = copy(hout, hin, 5, {"sp_2": 1 - c})
    across.start()

    def outputs(h, state):
        cols = pl.ds(pl.multiple_of(h * HEAD, HEAD), HEAD)
        for n in range(3):
            u = n * 2 + h
            span = slice(n * CHUNK, (n + 1) * CHUNK)
            out = from_values[u] + mm(from_state[u], state)
            if n < 2:
                state = carried(state, maps[u])
            out = out * lax.rsqrt(jnp.mean(out * out, axis=1, keepdims=True) + EPSILON)
            gated = out * gain_ref[...] * silu(gate_ref[span, cols].astype(F32))
            mixed_ref[span, cols] = gated.astype(BF16)

    outputs(c, jnp.where(c == 0, state, later))
    across.wait()
    outputs(1 - c, hin[...].astype(F32))

    @pl.when(z < 7)
    def _():
        onward.wait_send()


def attention(q, k, v, gate, strength, decay, extra, rate, gain):
    vmem = pl.BlockSpec(memory_space=pltpu.VMEM)
    return pl.pallas_call(
        attention_kernel,
        name="attention",
        out_shape=jax.ShapeDtypeStruct(q.shape, BF16),
        in_specs=[vmem] * 9,
        out_specs=vmem,
        scratch_shapes=[
            pltpu.VMEM((6, HEAD, 2 * HEAD), F32),
            pltpu.VMEM((6, CHUNK, HEAD), BF16),
            pltpu.VMEM((6, CHUNK, HEAD), F32),
            pltpu.VMEM((2, HEAD, 2 * HEAD), F32),
            pltpu.VMEM((2, HEAD, 2 * HEAD), BF16),
            pltpu.VMEM((HEAD, 2 * HEAD), BF16),
            pltpu.VMEM((4, HEAD, 2 * HEAD), BF16),
            pltpu.VMEM((HEAD, HEAD), BF16),
            pltpu.VMEM((HEAD, HEAD), BF16),
            pltpu.VMEM((HEAD, HEAD), BF16),
            pltpu.VMEM((HEAD, HEAD), BF16),
            pltpu.SemaphoreType.DMA((6,)),
            pltpu.SemaphoreType.DMA((6,)),
        ],
        compiler_params=pltpu.CompilerParams(
            collective_id=0, has_side_effects=True, vmem_limit_bytes=40 * 1024 * 1024
        ),
    )(q, k, v, gate, strength, decay, extra, rate[:, None], gain[None, :])


def sent_together(arrays, axis, dim, along):
    widths = [a.shape[along] for a in arrays]
    both = jnp.concatenate(arrays, axis=along)
    out = lax.all_gather(both, axis, axis=dim, tiled=True)
    return tuple(jnp.split(out, [sum(widths[:k]) for k in range(1, len(widths))], axis=along))


def split_up(value, dim, size):
    before, after = (value.shape[:dim], value.shape[dim + 1 :])
    return jnp.moveaxis(value.reshape(*before, size, -1, *after), dim, 0)


def sent_and_summed(value, axis, dim):
    tiles = split_up(value, dim, lax.axis_size(axis))
    arrived = lax.all_to_all(tiles, axis, split_axis=0, concat_axis=0, tiled=True)
    return arrived.astype(jnp.float32).sum(axis=0)


def copy_for_each(value, axis):
    copies = jnp.broadcast_to(value, (lax.axis_size(axis), *value.shape))
    return lax.all_to_all(copies, axis, split_axis=0, concat_axis=0, tiled=True)


def in_order(tiles, dim):
    tiles = jnp.moveaxis(tiles, 0, dim)
    lengths = tiles.shape
    return tiles.reshape(*lengths[:dim], lengths[dim] * lengths[dim + 1], *lengths[dim + 2 :])


def gather_directly(value, axis, dim):
    tiles = copy_for_each(value, axis)
    return in_order(tiles, dim)


def rms_scale(tensor):
    return tensor * lax.rsqrt(jnp.mean(tensor * tensor, axis=-1, keepdims=True) + EPSILON)


def feed_forward(whole_rows, gate_matrix, up_matrix, down_matrix):
    gate_whole, up_whole = sent_together((gate_matrix, up_matrix), SP, 0, 1)
    gate_total = jnp.dot(whole_rows, gate_whole, preferred_element_type=jnp.float32)
    up_total = jnp.dot(whole_rows, up_whole, preferred_element_type=jnp.float32)
    hidden = (jax.nn.silu(gate_total) * up_total).astype(jnp.bfloat16)
    down_whole = lax.all_gather(down_matrix, SP, axis=1, tiled=True)
    return jnp.dot(hidden, down_whole, preferred_element_type=jnp.float32)


def body(
    stream,
    query_projected,
    key_projected,
    value_projected,
    gate_projected,
    strength_logits,
    decay_preactivation,
    extra_log_decay,
    head_decay_rate,
    head_norm_gain,
    head_output_matrix,
    feed_norm_gain,
    gate_matrix,
    up_matrix,
    down_matrix,
):
    mixed = attention(
        query_projected,
        key_projected,
        value_projected,
        gate_projected,
        strength_logits,
        decay_preactivation,
        extra_log_decay,
        head_decay_rate,
        head_norm_gain,
    )
    branch = sent_and_summed(
        jnp.dot(mixed, head_output_matrix, preferred_element_type=jnp.float32).astype(jnp.bfloat16),
        "tp",
        0,
    )
    residual_own = stream.astype(jnp.float32) + branch
    normed_own = (rms_scale(residual_own) * feed_norm_gain).astype(jnp.bfloat16)
    whole_rows = gather_directly(normed_own, "tp", 0)
    ffn_term = feed_forward(whole_rows, gate_matrix, up_matrix, down_matrix)
    ffn_own = sent_and_summed(ffn_term.astype(jnp.bfloat16), "tp", 0)
    return (residual_own + ffn_own).astype(jnp.bfloat16)


def solution(mesh):
    torus = Mesh(mesh.devices.reshape(8, 4, 2, mesh.shape["tp"]), ("sp_0", "sp_1", "sp_2", "tp"))
    in_specs = (
        P(SP_TP, None),
        P(SP, "tp"),
        P(SP, "tp"),
        P(SP, "tp"),
        P(SP, "tp"),
        P("tp", SP),
        P("tp", SP),
        P("tp", SP),
        P("tp"),
        P(),
        P("tp", None),
        P(),
        P(SP, "tp"),
        P(SP, "tp"),
        P("tp", SP),
    )
    out_specs = P(SP_TP, None)
    return jax.shard_map(body, mesh=torus, in_specs=in_specs, out_specs=out_specs, check_vma=False)
```

```python
import functools
import jax
import jax.numpy as jnp
from jax import lax
from jax.experimental import pallas as pl
from jax.experimental.pallas import tpu as pltpu
from jax.sharding import Mesh
from jax.sharding import PartitionSpec as P

HEAD = 128
CHUNK = 128
SP = ("sp_0", "sp_1", "sp_2")
SP_TP = ("sp_0", "sp_1", "sp_2", "tp")
EPSILON = 1e-06
F32 = jnp.float32
BF16 = jnp.bfloat16
HIGH = lax.Precision.HIGHEST
MESH = pl.DeviceIdType.MESH


def mm(a, b):
    return jnp.dot(a.astype(BF16), b.astype(BF16), preferred_element_type=F32)


def mm_nt(a, b):
    return lax.dot_general(a, b, (((1,), (1,)), ((), ())), preferred_element_type=F32)


def mm_tn(a, b):
    return lax.dot_general(
        a.astype(BF16), b.astype(BF16), (((0,), (0,)), ((), ())), preferred_element_type=F32
    )


def full(a, b):
    return jnp.dot(a, b, precision=HIGH, preferred_element_type=F32)


def full_nt(a, b):
    return lax.dot_general(
        a, b, (((1,), (1,)), ((), ())), precision=HIGH, preferred_element_type=F32
    )


def silu(x):
    return x / (1.0 + jnp.exp(-x))


def softplus(x):
    return jnp.maximum(x, 0.0) + jnp.log1p(jnp.exp(-jnp.abs(x)))


def unit_lower_inverses(lowers, row, col):
    inverses = []
    for lower in lowers:
        near = jnp.where((row >> 3) == (col >> 3), lower, 0.0)
        inverses.append((near, jnp.where(row == col, 1.0, 0.0) - near))
    squares = [full(d, d) for d, _ in inverses]
    inverses = [x + full(x, s) for (_, x), s in zip(inverses, squares)]
    squares = [full(s, s) for s in squares]
    inverses = [x + full(x, s) for x, s in zip(inverses, squares)]
    for level in (3, 4, 5, 6):
        between = ((row >> (level + 1)) == (col >> (level + 1))) & ((row >> level) != (col >> level))
        parts = [jnp.where(between, lower, 0.0) for lower in lowers]
        parts = [full(p, x) for p, x in zip(parts, inverses)]
        inverses = [x - full(x, p) for p, x in zip(parts, inverses)]
    return inverses


def local_part(
    q_ref, k_ref, v_ref, strength_ref, decay_ref, extra_ref, rate_ref, maps, from_state, from_values, tick
):
    row = lax.broadcasted_iota(jnp.int32, (CHUNK, CHUNK), 0)
    col = lax.broadcasted_iota(jnp.int32, (CHUNK, CHUNK), 1)
    eye = jnp.where(row == col, 1.0, 0.0)
    lower_ones = jnp.where(row >= col, 1.0, 0.0)
    upper_ones = jnp.where(row <= col, 1.0, 0.0)
    padding = jnp.zeros((6, CHUNK), F32)

    def chunk(c, carry):
        span = pl.ds(pl.multiple_of(c * CHUNK, CHUNK), CHUNK)
        logs = -rate_ref[...] * softplus(decay_ref[:, span].astype(F32)) + extra_ref[:, span]
        beta = 1.0 / (1.0 + jnp.exp(-strength_ref[:, span].astype(F32)))
        logs = jnp.concatenate([logs, padding], axis=0)
        beta = jnp.concatenate([beta, padding], axis=0)
        sums_row = full(logs, upper_ones)
        sums_col = full_nt(lower_ones, logs)
        beta_col = full_nt(eye, beta)
        lowers, scores, rights, keys, queries, closings = [], [], [], [], [], []
        for h in range(2):
            cols = slice(h * HEAD, (h + 1) * HEAD)
            k = k_ref[span, cols]
            q = q_ref[span, cols]
            kf, qf, vf = k.astype(F32), q.astype(F32), v_ref[span, cols].astype(F32)
            squares = kf * kf
            k_col = lax.rsqrt(jnp.sum(squares, axis=1, keepdims=True) + EPSILON)
            k_row = lax.rsqrt(full_nt(jnp.ones((8, HEAD), F32), squares)[0:1] + EPSILON)
            q_col = lax.rsqrt(jnp.sum(qf * qf, axis=1, keepdims=True) + EPSILON) * HEAD ** (-0.5)
            s_col, s_row, b_col = sums_col[:, h : h + 1], sums_row[h : h + 1], beta_col[:, h : h + 1]
            closing = s_row[:, CHUNK - 1 :]
            damping = jnp.exp(jnp.minimum(s_col - s_row, 0.0)) * k_row
            lowers.append(jnp.where(row > col, mm_nt(k, k) * damping * (b_col * k_col), 0.0))
            scores.append(jnp.where(row >= col, mm_nt(q, k) * damping * q_col, 0.0))
            opening = jnp.exp(s_col)
            rights.append(
                jnp.concatenate([kf * (b_col * k_col * opening), vf * b_col], axis=1)
            )
            keys.append(kf * (k_col * jnp.exp(closing - s_col)))
            queries.append(qf * (q_col * opening))
            closings.append(jnp.exp(closing) - 1.0)
        inverses = unit_lower_inverses(lowers, row, col)
        solved = [r + mm(x - eye, r) for x, r in zip(inverses, rights)]
        for h in range(2):
            u = c * 2 + h
            change = mm_tn(keys[h], solved[h])
            maps[u, :, :HEAD] = closings[h] * eye - change[:, :HEAD]
            maps[u, :, HEAD:] = change[:, HEAD:]
            out = mm(scores[h], solved[h])
            from_state[u] = (queries[h] - out[:, :HEAD]).astype(BF16)
            from_values[u] = out[:, HEAD:]
        tick(c + 1)
        return carry

    lax.fori_loop(0, 3, chunk, 0)


def joined(earlier, later):
    return earlier + later + mm(later[:, :HEAD], earlier)


def carried(state, pair):
    return state + pair[:, HEAD:] + mm(pair[:, :HEAD], state)


RINGS = ((0, 1, 16), (0, -1, 15), (1, 1, 16), (1, -1, 15))
PIECES = (
    ((0, 0), (0, 16), (2, 0)),
    ((1, 0), (1, 16), (2, 16)),
)
PIECE = 16


def place_of(cycle, position):
    run, step = position // 4, position % 4
    if cycle == 0:
        return run, (step + 8 - run) % 4
    return (3 * run + step) % 8, run % 4


def positions(z, y):
    first = 4 * z + (y + z) % 4
    step = (z + 16 - 3 * y) % 8
    second = jnp.where(step < 4, 4 * y + step, 4 * (y + 4) + (step + 4) % 8)
    return first, second


class Gather:
    def __init__(self, z, y, c, shards, wholes, sems):
        self.c, self.shards, self.wholes = c, shards, wholes
        self.ring_send, self.sib_send, self.ring_recv, self.sib_recv = sems
        self.own = positions(z, y)
        self.here = z * 4 + y
        self.targets = []
        for cycle, way, _ in RINGS:
            to_z, to_y = place_of(cycle, (self.own[cycle] + 32 + way) % 32)
            self.targets.append({"sp_0": to_z, "sp_1": to_y})

    def block(self, matrix, first, where):
        return self.wholes[matrix].at[where, self.c, pl.ds(first, PIECE)]

    def onward(self, ring, piece, step, src, where):
        matrix, first = PIECES[RINGS[ring][0]][piece]
        return pltpu.make_async_remote_copy(
            src_ref=src,
            dst_ref=self.block(matrix, first, where),
            send_sem=self.ring_send.at[matrix],
            recv_sem=self.ring_recv.at[ring, piece, step],
            device_id=self.targets[ring],
            device_id_type=MESH,
        )

    def across(self, src, matrix, dst):
        return pltpu.make_async_remote_copy(
            src_ref=src,
            dst_ref=dst,
            send_sem=self.sib_send.at[matrix],
            recv_sem=self.sib_recv.at[matrix],
            device_id={"sp_2": 1 - self.c},
            device_id_type=MESH,
        )

    def start(self):
        for piece in range(3):
            for ring in range(4):
                matrix, first = PIECES[RINGS[ring][0]][piece]
                src = self.shards[matrix].at[pl.ds(first, PIECE)]
                self.onward(ring, piece, 0, src, self.here).start()
        for matrix in range(3):
            self.across(
                self.shards[matrix], matrix, self.wholes[matrix].at[self.here, self.c]
            ).start()
        for matrix in range(3):
            self.wholes[matrix][self.here, self.c] = self.shards[matrix][...]

    def tick(self, step):
        for piece in range(3):
            for ring in range(4):
                cycle, way, last = RINGS[ring]
                matrix, first = PIECES[cycle][piece]

                def move():
                    z, y = place_of(cycle, (self.own[cycle] + 32 - way * step) % 32)
                    where = z * 4 + y
                    block = self.block(matrix, first, where)
                    self.onward(ring, piece, step - 1, block, where).wait_recv()

                    @pl.when(step < last)
                    def _():
                        self.onward(ring, piece, step, block, where).start()

                    self.across(block, matrix, block).start()

                if last == 16:
                    move()
                else:
                    pl.when(step <= last)(move)

    def finish(self):
        for matrix in range(3):
            sibling = self.wholes[matrix].at[:, 1 - self.c]
            self.across(sibling, matrix, sibling).wait()
        for matrix in range(3):
            most = self.wholes[matrix].at[pl.ds(0, 31), self.c]
            pltpu.make_async_remote_copy(
                src_ref=most,
                dst_ref=most,
                send_sem=self.ring_send.at[matrix],
                recv_sem=self.ring_recv.at[0, 0, 0],
                device_id=self.targets[0],
                device_id_type=MESH,
            ).wait_send()


def attention_kernel(
    q_ref,
    k_ref,
    v_ref,
    gate_ref,
    strength_ref,
    decay_ref,
    extra_ref,
    rate_ref,
    gain_ref,
    gate_shard,
    up_shard,
    down_shard,
    mixed_ref,
    gate_whole,
    up_whole,
    down_whole,
    maps,
    from_state,
    from_values,
    totals,
    pair,
    sib,
    chip,
    zin1,
    zin2,
    zin4,
    zout1,
    zout2,
    zout4,
    hin,
    hout,
    send_sem,
    recv_sem,
    ring_send,
    sib_send,
    ring_recv,
    sib_recv,
):
    z, y, c = lax.axis_index("sp_0"), lax.axis_index("sp_1"), lax.axis_index("sp_2")
    for ref in (zin1, zin2, zin4):
        ref[...] = jnp.zeros_like(ref)
    barrier = pltpu.get_barrier_semaphore()
    peers = [{"sp_2": 1 - c}]
    peers += [{"sp_1": lax.rem(y + d, 4)} for d in (1, 2, 3)]
    peers += [{"sp_0": lax.rem(z + d, 8)} for d in (1, 2, 4, 6, 7)]
    for peer in peers:
        pl.semaphore_signal(barrier, inc=1, device_id=peer, device_id_type=MESH)
    pl.semaphore_wait(barrier, len(peers))

    gather = Gather(
        z,
        y,
        c,
        (gate_shard, up_shard, down_shard),
        (gate_whole, up_whole, down_whole),
        (ring_send, sib_send, ring_recv, sib_recv),
    )
    gather.start()

    def copy(src, dst, slot, peer):
        return pltpu.make_async_remote_copy(
            src_ref=src,
            dst_ref=dst,
            send_sem=send_sem.at[slot],
            recv_sem=recv_sem.at[slot],
            device_id=peer,
            device_id_type=MESH,
        )

    local_part(
        q_ref,
        k_ref,
        v_ref,
        strength_ref,
        decay_ref,
        extra_ref,
        rate_ref,
        maps,
        from_state,
        from_values,
        gather.tick,
    )
    for h in range(2):
        total = joined(joined(maps[h], maps[2 + h]), maps[4 + h])
        totals[h] = total
        pair[h] = total.astype(BF16)

    to_sib = copy(pair.at[1 - c], sib, 0, {"sp_2": 1 - c})
    to_sib.start()
    to_sib.wait()
    own, other = totals[c], sib[...].astype(F32)
    first = jnp.where(c == 0, own, other)
    chip[y] = joined(first, jnp.where(c == 0, other, own)).astype(BF16)
    totals[1] = first

    sends = []
    for d in (1, 2, 3):
        sends.append(copy(chip.at[y], chip.at[y], d, {"sp_1": lax.rem(y + d, 4)}))
        sends[-1].start()
    gather.tick(4)
    for d in (1, 2, 3):
        source = lax.rem(y + 4 - d, 4)
        copy(chip.at[source], chip.at[source], d, {"sp_1": lax.rem(y + d, 4)}).wait_recv()
    total = chip[0].astype(F32)
    before = jnp.where(y == 0, 0.0, total)
    for s in (1, 2, 3):
        total = joined(total, chip[s].astype(F32))
        if s < 3:
            before = jnp.where(y > s, total, before)
    for send in sends:
        send.wait_send()

    totals[0] = before
    earlier = jnp.zeros((HEAD, 2 * HEAD), F32)
    hops = ((1, zout1, zin1), (2, zout2, zin2), (4, zout4, zin4))
    for n, (d, out, arrived) in enumerate(hops):
        out[...] = total[:, (2 * HEAD - out.shape[1]) :].astype(BF16)
        hop = copy(out, arrived, 4 + n, {"sp_0": lax.rem(z + d, 8)})

        @pl.when(z + d < 8)
        def _():
            hop.start()

        gather.tick(5 + n)

        @pl.when(z >= d)
        def _():
            hop.wait_recv()

        came = arrived[...].astype(F32)
        if d < 4:
            earlier = joined(came, earlier)
            total = joined(came, total)
        else:
            state = carried(came, earlier)

        @pl.when(z + d < 8)
        def _():
            hop.wait_send()

    state = carried(state, totals[0])
    later = carried(state, totals[1])
    hout[...] = jnp.where(c == 0, later, state).astype(BF16)
    across = copy(hout, hin, 7, {"sp_2": 1 - c})
    across.start()

    def outputs(h, state):
        cols = pl.ds(pl.multiple_of(h * HEAD, HEAD), HEAD)
        for n in range(3):
            u = n * 2 + h
            span = slice(n * CHUNK, (n + 1) * CHUNK)
            out = from_values[u] + mm(from_state[u], state)
            if n < 2:
                state = carried(state, maps[u])
            out = out * lax.rsqrt(jnp.mean(out * out, axis=1, keepdims=True) + EPSILON)
            gated = out * gain_ref[...] * silu(gate_ref[span, cols].astype(F32))
            mixed_ref[span, cols] = gated.astype(BF16)

    outputs(c, jnp.where(c == 0, state, later))
    across.wait()
    outputs(1 - c, hin[...].astype(F32))

    def rest(step, carry):
        gather.tick(step)
        return carry

    lax.fori_loop(8, 17, rest, 0)
    gather.finish()


def attention(q, k, v, gate, strength, decay, extra, rate, gain, gate_shard, up_shard, down_shard):
    vmem = pl.BlockSpec(memory_space=pltpu.VMEM)
    whole = jax.ShapeDtypeStruct((32, 2, *gate_shard.shape), BF16)
    mixed, *wholes = pl.pallas_call(
        attention_kernel,
        name="attention",
        out_shape=[jax.ShapeDtypeStruct(q.shape, BF16)] + [whole] * 3,
        in_specs=[vmem] * 12,
        out_specs=[vmem] * 4,
        scratch_shapes=[
            pltpu.VMEM((6, HEAD, 2 * HEAD), F32),
            pltpu.VMEM((6, CHUNK, HEAD), BF16),
            pltpu.VMEM((6, CHUNK, HEAD), F32),
            pltpu.VMEM((2, HEAD, 2 * HEAD), F32),
            pltpu.VMEM((2, HEAD, 2 * HEAD), BF16),
            pltpu.VMEM((HEAD, 2 * HEAD), BF16),
            pltpu.VMEM((4, HEAD, 2 * HEAD), BF16),
            pltpu.VMEM((HEAD, 2 * HEAD), BF16),
            pltpu.VMEM((HEAD, 2 * HEAD), BF16),
            pltpu.VMEM((HEAD, HEAD), BF16),
            pltpu.VMEM((HEAD, 2 * HEAD), BF16),
            pltpu.VMEM((HEAD, 2 * HEAD), BF16),
            pltpu.VMEM((HEAD, HEAD), BF16),
            pltpu.VMEM((HEAD, HEAD), BF16),
            pltpu.VMEM((HEAD, HEAD), BF16),
            pltpu.SemaphoreType.DMA((8,)),
            pltpu.SemaphoreType.DMA((8,)),
            pltpu.SemaphoreType.DMA((3,)),
            pltpu.SemaphoreType.DMA((3,)),
            pltpu.SemaphoreType.DMA((4, 3, 16)),
            pltpu.SemaphoreType.DMA((3,)),
        ],
        compiler_params=pltpu.CompilerParams(
            collective_id=0, has_side_effects=True, vmem_limit_bytes=56 * 1024 * 1024
        ),
    )(q, k, v, gate, strength, decay, extra, rate[:, None], gain[None, :], gate_shard, up_shard, down_shard)
    return mixed, *(w.reshape(-1, w.shape[-1]) for w in wholes)


def split_up(value, dim, size):
    before, after = (value.shape[:dim], value.shape[dim + 1 :])
    return jnp.moveaxis(value.reshape(*before, size, -1, *after), dim, 0)


def sent_and_summed(value, axis, dim):
    tiles = split_up(value, dim, lax.axis_size(axis))
    arrived = lax.all_to_all(tiles, axis, split_axis=0, concat_axis=0, tiled=True)
    return arrived.astype(jnp.float32).sum(axis=0)


def copy_for_each(value, axis):
    copies = jnp.broadcast_to(value, (lax.axis_size(axis), *value.shape))
    return lax.all_to_all(copies, axis, split_axis=0, concat_axis=0, tiled=True)


def in_order(tiles, dim):
    tiles = jnp.moveaxis(tiles, 0, dim)
    lengths = tiles.shape
    return tiles.reshape(*lengths[:dim], lengths[dim] * lengths[dim + 1], *lengths[dim + 2 :])


def gather_directly(value, axis, dim):
    tiles = copy_for_each(value, axis)
    return in_order(tiles, dim)


def rms_scale(tensor):
    return tensor * lax.rsqrt(jnp.mean(tensor * tensor, axis=-1, keepdims=True) + EPSILON)


def feed_forward(whole_rows, gate_whole, up_whole, down_whole):
    gate_total = jnp.dot(whole_rows, gate_whole, preferred_element_type=jnp.float32)
    up_total = jnp.dot(whole_rows, up_whole, preferred_element_type=jnp.float32)
    hidden = (jax.nn.silu(gate_total) * up_total).astype(jnp.bfloat16)
    return lax.dot_general(hidden, down_whole, (((1,), (1,)), ((), ())), preferred_element_type=jnp.float32)


def body(
    stream,
    query_projected,
    key_projected,
    value_projected,
    gate_projected,
    strength_logits,
    decay_preactivation,
    extra_log_decay,
    head_decay_rate,
    head_norm_gain,
    head_output_matrix,
    feed_norm_gain,
    gate_matrix,
    up_matrix,
    down_matrix,
):
    mixed, gate_whole, up_whole, down_whole = attention(
        query_projected,
        key_projected,
        value_projected,
        gate_projected,
        strength_logits,
        decay_preactivation,
        extra_log_decay,
        head_decay_rate,
        head_norm_gain,
        gate_matrix,
        up_matrix,
        down_matrix.T,
    )
    branch = sent_and_summed(
        jnp.dot(mixed, head_output_matrix, preferred_element_type=jnp.float32).astype(jnp.bfloat16),
        "tp",
        0,
    )
    residual_own = stream.astype(jnp.float32) + branch
    normed_own = (rms_scale(residual_own) * feed_norm_gain).astype(jnp.bfloat16)
    whole_rows = gather_directly(normed_own, "tp", 0)
    ffn_term = feed_forward(whole_rows, gate_whole, up_whole, down_whole)
    ffn_own = sent_and_summed(ffn_term.astype(jnp.bfloat16), "tp", 0)
    return (residual_own + ffn_own).astype(jnp.bfloat16)


def solution(mesh):
    torus = Mesh(mesh.devices.reshape(8, 4, 2, mesh.shape["tp"]), ("sp_0", "sp_1", "sp_2", "tp"))
    in_specs = (
        P(SP_TP, None),
        P(SP, "tp"),
        P(SP, "tp"),
        P(SP, "tp"),
        P(SP, "tp"),
        P("tp", SP),
        P("tp", SP),
        P("tp", SP),
        P("tp"),
        P(),
        P("tp", None),
        P(),
        P(SP, "tp"),
        P(SP, "tp"),
        P("tp", SP),
    )
    out_specs = P(SP_TP, None)
    return jax.shard_map(body, mesh=torus, in_specs=in_specs, out_specs=out_specs, check_vma=False)
```

```python
import functools
import jax
import jax.numpy as jnp
from jax import lax
from jax.experimental import pallas as pl
from jax.experimental.pallas import tpu as pltpu
from jax.sharding import Mesh
from jax.sharding import PartitionSpec as P

HEAD = 128
CHUNK = 128
SP = ("sp_0", "sp_1", "sp_2")
SP_TP = ("sp_0", "sp_1", "sp_2", "tp")
EPSILON = 1e-06
F32 = jnp.float32
BF16 = jnp.bfloat16
HIGH = lax.Precision.HIGHEST
MESH = pl.DeviceIdType.MESH


def mm(a, b):
    return jnp.dot(a.astype(BF16), b.astype(BF16), preferred_element_type=F32)


def mm_nt(a, b):
    return lax.dot_general(a, b, (((1,), (1,)), ((), ())), preferred_element_type=F32)


def mm_tn(a, b):
    return lax.dot_general(
        a.astype(BF16), b.astype(BF16), (((0,), (0,)), ((), ())), preferred_element_type=F32
    )


def full(a, b):
    return jnp.dot(a, b, precision=HIGH, preferred_element_type=F32)


def full_nt(a, b):
    return lax.dot_general(
        a, b, (((1,), (1,)), ((), ())), precision=HIGH, preferred_element_type=F32
    )


def silu(x):
    return x / (1.0 + jnp.exp(-x))


def softplus(x):
    return jnp.maximum(x, 0.0) + jnp.log1p(jnp.exp(-jnp.abs(x)))


def unit_lower_inverses(lowers, row, col):
    inverses = []
    for lower in lowers:
        near = jnp.where((row >> 3) == (col >> 3), lower, 0.0)
        inverses.append((near, jnp.where(row == col, 1.0, 0.0) - near))
    squares = [full(d, d) for d, _ in inverses]
    inverses = [x + full(x, s) for (_, x), s in zip(inverses, squares)]
    squares = [full(s, s) for s in squares]
    inverses = [x + full(x, s) for x, s in zip(inverses, squares)]
    for level in (3, 4, 5, 6):
        between = ((row >> (level + 1)) == (col >> (level + 1))) & ((row >> level) != (col >> level))
        parts = [jnp.where(between, lower, 0.0) for lower in lowers]
        parts = [full(p, x) for p, x in zip(parts, inverses)]
        inverses = [x - full(x, p) for p, x in zip(parts, inverses)]
    return inverses


def local_chunk(
    c, q_ref, k_ref, v_ref, strength_ref, decay_ref, extra_ref, rate_ref, maps, from_state, from_values
):
    row = lax.broadcasted_iota(jnp.int32, (CHUNK, CHUNK), 0)
    col = lax.broadcasted_iota(jnp.int32, (CHUNK, CHUNK), 1)
    eye = jnp.where(row == col, 1.0, 0.0)
    lower_ones = jnp.where(row >= col, 1.0, 0.0)
    upper_ones = jnp.where(row <= col, 1.0, 0.0)
    padding = jnp.zeros((6, CHUNK), F32)
    span = pl.ds(pl.multiple_of(c * CHUNK, CHUNK), CHUNK)
    logs = -rate_ref[...] * softplus(decay_ref[:, span].astype(F32)) + extra_ref[:, span]
    beta = 1.0 / (1.0 + jnp.exp(-strength_ref[:, span].astype(F32)))
    logs = jnp.concatenate([logs, padding], axis=0)
    beta = jnp.concatenate([beta, padding], axis=0)
    sums_row = full(logs, upper_ones)
    sums_col = full_nt(lower_ones, logs)
    beta_col = full_nt(eye, beta)
    lowers, scores, rights, keys, queries, closings = [], [], [], [], [], []
    for h in range(2):
        cols = slice(h * HEAD, (h + 1) * HEAD)
        k = k_ref[span, cols]
        q = q_ref[span, cols]
        kf, qf, vf = k.astype(F32), q.astype(F32), v_ref[span, cols].astype(F32)
        squares = kf * kf
        k_col = lax.rsqrt(jnp.sum(squares, axis=1, keepdims=True) + EPSILON)
        k_row = lax.rsqrt(full_nt(jnp.ones((8, HEAD), F32), squares)[0:1] + EPSILON)
        q_col = lax.rsqrt(jnp.sum(qf * qf, axis=1, keepdims=True) + EPSILON) * HEAD ** (-0.5)
        s_col, s_row, b_col = sums_col[:, h : h + 1], sums_row[h : h + 1], beta_col[:, h : h + 1]
        closing = s_row[:, CHUNK - 1 :]
        damping = jnp.exp(jnp.minimum(s_col - s_row, 0.0)) * k_row
        lowers.append(jnp.where(row > col, mm_nt(k, k) * damping * (b_col * k_col), 0.0))
        scores.append(jnp.where(row >= col, mm_nt(q, k) * damping * q_col, 0.0))
        opening = jnp.exp(s_col)
        rights.append(
            jnp.concatenate([kf * (b_col * k_col * opening), vf * b_col], axis=1)
        )
        keys.append(kf * (k_col * jnp.exp(closing - s_col)))
        queries.append(qf * (q_col * opening))
        closings.append(jnp.exp(closing) - 1.0)
    inverses = unit_lower_inverses(lowers, row, col)
    solved = [r + mm(x - eye, r) for x, r in zip(inverses, rights)]
    for h in range(2):
        u = c * 2 + h
        change = mm_tn(keys[h], solved[h])
        maps[u, :, :HEAD] = closings[h] * eye - change[:, :HEAD]
        maps[u, :, HEAD:] = change[:, HEAD:]
        out = mm(scores[h], solved[h])
        from_state[u] = (queries[h] - out[:, :HEAD]).astype(BF16)
        from_values[u] = out[:, HEAD:]


def joined(earlier, later):
    return earlier + later + mm(later[:, :HEAD], earlier)


def carried(state, pair):
    return state + pair[:, HEAD:] + mm(pair[:, :HEAD], state)


A_ROWS = (0, 64)
B_ROWS = (64, 32)


def halves(rows):
    first, count = rows
    return (first, count // 2), (first + count // 2, count // 2)


def sides(rows, offsets, place):
    if len(offsets) == 2:
        return [(place(offsets[0]), rows)], [(place(offsets[1]), rows)]
    low, high = halves(rows)
    return [(place(offsets[0]), low)], [(place(offsets[0]), high)]


class Gather:
    def __init__(self, z, y, c, shard, whole, sems):
        self.z, self.y, self.c, self.shard, self.whole = z, y, c, shard, whole
        self.ring_send, self.sib_send, self.ring_recv, self.sib_recv = sems
        self.used = 0
        self.moves = {}
        self.groups_a = [(0,), (-1, 1), (-2, 2), (-3, 3), (-4,)]
        self.groups_b = [(0,), (-1, 1), (2,)]
        for s in (1, 2, 3):
            for way in (1, -1):
                self.plan("az", s, way, 0, [((-way * s, 0), A_ROWS)])
        for way, blocks in zip((1, -1), sides(A_ROWS, (-4,), lambda o: (o, 0))):
            self.plan("az", 4, way, 0, blocks)
        for g, offsets in enumerate(self.groups_a):
            for way in (1, -1):
                self.plan("ay", (g, 1), way, 1, [((o, -way), A_ROWS) for o in offsets])
            for way, blocks in zip((1, -1), sides(A_ROWS, offsets, lambda o: (o, 2))):
                self.plan("ay", (g, 2), way, 1, blocks)
        for way in (1, -1):
            self.plan("by", 1, way, 1, [((0, -way), B_ROWS)])
        for way, blocks in zip((1, -1), sides(B_ROWS, (2,), lambda o: (0, o))):
            self.plan("by", 2, way, 1, blocks)
        for g, offsets in enumerate(self.groups_b):
            for s in (1, 2, 3):
                for way in (1, -1):
                    self.plan("bz", (g, s), way, 0, [((-way * s, o), B_ROWS) for o in offsets])
            for way, blocks in zip((1, -1), sides(B_ROWS, offsets, lambda o: (4, o))):
                self.plan("bz", (g, 4), way, 0, blocks)

    def plan(self, flow, step, way, axis, blocks):
        entries = []
        for place, rows in blocks:
            entries.append((place, rows, self.used))
            self.used += 1
        self.moves[flow, step, way] = (axis, entries)

    def block(self, place, rows):
        z = (self.z + place[0] + 8) % 8
        y = (self.y + place[1] + 8) % 4
        return self.whole.at[z * 4 + y, self.c, pl.ds(*rows)]

    def copy(self, axis, way, place, rows, sem, src, dst):
        name, size, at = (("sp_0", 8, self.z), ("sp_1", 4, self.y))[axis]
        return pltpu.make_async_remote_copy(
            src_ref=src,
            dst_ref=dst,
            send_sem=self.ring_send,
            recv_sem=self.ring_recv.at[sem],
            device_id={name: (at + way + size) % size},
            device_id_type=MESH,
        )

    def send(self, flow, step):
        for way in (1, -1):
            axis, entries = self.moves[flow, step, way]
            for place, rows, sem in entries:
                shift = (place[0] + way, place[1]) if axis == 0 else (place[0], place[1] + way)
                dst = self.block(shift, rows)
                own = shift[0] % 8 == 0 and shift[1] % 4 == 0
                src = self.shard.at[pl.ds(*rows)] if own else dst
                self.copy(axis, way, place, rows, sem, src, dst).start()

    def receive(self, flow, step):
        for way in (1, -1):
            axis, entries = self.moves[flow, step, way]
            for place, rows, sem in entries:
                block = self.block(place, rows)
                self.copy(axis, way, place, rows, sem, block, block).wait_recv()
                self.across(block, block).start()

    def across(self, src, dst):
        return pltpu.make_async_remote_copy(
            src_ref=src,
            dst_ref=dst,
            send_sem=self.sib_send,
            recv_sem=self.sib_recv,
            device_id={"sp_2": 1 - self.c},
            device_id_type=MESH,
        )

    def start(self):
        self.send("by", 1)
        self.send("az", 1)
        self.send("ay", (0, 1))
        self.send("bz", (0, 1))
        here = self.z * 4 + self.y
        self.across(self.shard, self.whole.at[here, self.c]).start()
        self.whole[here, self.c] = self.shard[...]

    def az(self, s):
        self.receive("az", s)
        if s < 4:
            self.send("az", s + 1)
        self.send("ay", (s, 1))

    def ay(self, g, s):
        self.receive("ay", (g, s))
        if s == 1:
            self.send("ay", (g, 2))

    def by(self, s):
        self.receive("by", s)
        if s == 1:
            self.send("by", 2)
        self.send("bz", (s, 1))

    def bz(self, g, s):
        self.receive("bz", (g, s))
        if s < 4:
            self.send("bz", (g, s + 1))

    def events(self):
        az, ay, by, bz = self.az, self.ay, self.by, self.bz
        return [
            (by, 1), (az, 1), (bz, 0, 1), (ay, 0, 1),
            (by, 2), (az, 2), (bz, 0, 2), (bz, 1, 1),
            (ay, 1, 1), (ay, 0, 2), (az, 3), (bz, 0, 3), (bz, 2, 1), (bz, 1, 2),
            (az, 4), (ay, 1, 2), (ay, 2, 1), (bz, 0, 4), (bz, 2, 2), (bz, 1, 3),
            (ay, 2, 2), (ay, 3, 1), (bz, 2, 3), (bz, 1, 4),
            (ay, 3, 2), (ay, 4, 1), (bz, 2, 4),
            (ay, 4, 2),
        ]

    def finish(self):
        sibling = self.whole.at[:, 1 - self.c]
        self.across(sibling, sibling).wait()
        most = self.whole.at[pl.ds(0, 31), self.c]
        self.copy(0, 1, None, None, 0, most, most).wait_send()


FAR, RIGHT, LEFT, OWN = range(4)
TOK = 96
WIDE = 256


def layer_kernel(
    q_ref,
    k_ref,
    v_ref,
    gate_ref,
    strength_ref,
    decay_ref,
    extra_ref,
    rate_ref,
    gain_ref,
    stream_ref,
    head_ref,
    feed_gain_ref,
    shard,
    result_ref,
    maps,
    from_state,
    from_values,
    totals,
    pair,
    sib,
    chip,
    zin1,
    zin2,
    zin4,
    zout1,
    zout2,
    zout4,
    hin,
    hout,
    mixed,
    mixed_in,
    head_whole,
    residual,
    rows,
    hidden,
    whole,
    far_out,
    relayed,
    outgoing,
    incoming,
    send_sem,
    recv_sem,
    ring_send,
    sib_send,
    ring_recv,
    sib_recv,
):
    z, y, c = lax.axis_index("sp_0"), lax.axis_index("sp_1"), lax.axis_index("sp_2")
    x = lax.axis_index("tp")
    for ref in (zin1, zin2, zin4):
        ref[...] = jnp.zeros_like(ref)
    to_sibling = {"sp_2": 1 - c}
    to_right, to_left, to_far = ({"tp": lax.rem(x + d, 4)} for d in (1, 3, 2))
    barrier = pltpu.get_barrier_semaphore()
    peers = [to_sibling, to_right, to_left, to_far]
    peers += [{"sp_1": lax.rem(y + d, 4)} for d in (1, 2, 3)]
    peers += [{"sp_0": lax.rem(z + d, 8)} for d in (1, 2, 4, 6, 7)]
    for peer in peers:
        pl.semaphore_signal(barrier, inc=1, device_id=peer, device_id_type=MESH)
    pl.semaphore_wait(barrier, len(peers))

    gather = Gather(z, y, c, shard, whole, (ring_send, sib_send, ring_recv, sib_recv))
    gather.start()
    events = iter(gather.events())

    def pump(count):
        for _ in range(count):
            event = next(events, None)
            if event is not None:
                event[0](*event[1:])

    slots = iter(range(64))

    def copy(src, dst, peer):
        slot = next(slots)
        return pltpu.make_async_remote_copy(
            src_ref=src,
            dst_ref=dst,
            send_sem=send_sem.at[slot],
            recv_sem=recv_sem.at[slot],
            device_id=peer,
            device_id_type=MESH,
        )

    half = head_ref.at[pl.ds(pl.multiple_of(c * HEAD, HEAD), HEAD)]
    head_near = [
        copy(half, head_whole.at[LEFT, c], to_right),
        copy(half, head_whole.at[RIGHT, c], to_left),
    ]
    for move in head_near:
        move.start()
    low, high = pl.ds(0, HEAD // 2), pl.ds(HEAD // 2, HEAD // 2)
    head_far = [
        copy(head_whole.at[LEFT, c, low], head_whole.at[FAR, c, low], to_right),
        copy(head_whole.at[RIGHT, c, high], head_whole.at[FAR, c, high], to_left),
    ]
    head_sib = [
        copy(head_whole.at[side, c], head_whole.at[side, c], to_sibling) for side in (FAR, RIGHT, LEFT)
    ]

    for n in range(3):
        local_chunk(
            n,
            q_ref,
            k_ref,
            v_ref,
            strength_ref,
            decay_ref,
            extra_ref,
            rate_ref,
            maps,
            from_state,
            from_values,
        )
        pump(PUMPS[n])
    for h in range(2):
        total = joined(joined(maps[h], maps[2 + h]), maps[4 + h])
        totals[h] = total
        pair[h] = total.astype(BF16)

    to_sib = copy(pair.at[1 - c], sib, to_sibling)
    to_sib.start()
    to_sib.wait()
    own, other = totals[c], sib[...].astype(F32)
    first = jnp.where(c == 0, own, other)
    chip[y] = joined(first, jnp.where(c == 0, other, own)).astype(BF16)
    totals[1] = first

    sends = []
    for d in (1, 2, 3):
        sends.append(copy(chip.at[y], chip.at[y], {"sp_1": lax.rem(y + d, 4)}))
        sends[-1].start()
    pump(PUMPS[3])
    for d in (1, 2, 3):
        sends[d - 1].wait()
    total = chip[0].astype(F32)
    before = jnp.where(y == 0, 0.0, total)
    for s in (1, 2, 3):
        total = joined(total, chip[s].astype(F32))
        if s < 3:
            before = jnp.where(y > s, total, before)

    totals[0] = before
    earlier = jnp.zeros((HEAD, 2 * HEAD), F32)
    for n, (d, out, arrived) in enumerate(((1, zout1, zin1), (2, zout2, zin2), (4, zout4, zin4))):
        out[...] = total[:, (2 * HEAD - out.shape[1]) :].astype(BF16)
        hop = copy(out, arrived, {"sp_0": lax.rem(z + d, 8)})

        @pl.when(z + d < 8)
        def _():
            hop.start()

        pump(PUMPS[4 + n])

        @pl.when(z >= d)
        def _():
            hop.wait_recv()

        came = arrived[...].astype(F32)
        if d < 4:
            earlier = joined(came, earlier)
            total = joined(came, total)
        else:
            state = carried(came, earlier)

        @pl.when(z + d < 8)
        def _():
            hop.wait_send()

        if n == 0:
            for near, far in zip(head_near, head_far):
                near.wait_recv()
                far.start()
            head_sib[2].start()
            head_sib[1].start()
        if n == 2:
            for far in head_far:
                far.wait_recv()
            head_sib[0].start()

    state = carried(state, totals[0])
    later = carried(state, totals[1])
    hout[...] = jnp.where(c == 0, later, state).astype(BF16)
    across = copy(hout, hin, to_sibling)
    across.start()

    def outputs(h, state):
        cols = pl.ds(pl.multiple_of(h * HEAD, HEAD), HEAD)
        for n in range(3):
            u = n * 2 + h
            span = slice(n * CHUNK, (n + 1) * CHUNK)
            out = from_values[u] + mm(from_state[u], state)
            if n < 2:
                state = carried(state, maps[u])
            out = out * lax.rsqrt(jnp.mean(out * out, axis=1, keepdims=True) + EPSILON)
            gated = out * gain_ref[...] * silu(gate_ref[span, cols].astype(F32))
            mixed[span, cols] = gated.astype(BF16)

    outputs(c, jnp.where(c == 0, state, later))
    across.wait()
    outputs(1 - c, hin[...].astype(F32))

    def rows_of(d):
        return pl.ds(pl.multiple_of(lax.rem(x + d, 4) * TOK, TOK), TOK)

    exchange = [
        copy(mixed.at[rows_of(2)], mixed_in.at[FAR], to_far),
        copy(mixed.at[rows_of(1)], mixed_in.at[LEFT], to_right),
        copy(mixed.at[rows_of(3)], mixed_in.at[RIGHT], to_left),
    ]
    for move in exchange:
        move.start()
    pump(PUMPS[7])
    mixed_in[OWN] = mixed[rows_of(0), :]
    for move in head_sib:
        move.wait()
    head_whole[OWN] = head_ref[...].reshape(2, HEAD, -1)
    for move in exchange:
        move.wait()

    def project(n, squares):
        cols = pl.ds(pl.multiple_of(n * WIDE, WIDE), WIDE)
        tile = stream_ref[:, cols].astype(F32)
        for side in range(4):
            matrix = head_whole[side, :, :, cols].reshape(2 * HEAD, WIDE)
            tile = tile + jnp.dot(mixed_in[side], matrix, preferred_element_type=F32)
        residual[:, cols] = tile
        return squares + jnp.sum(tile * tile, axis=1, keepdims=True)

    width = residual.shape[1]
    squares = lax.fori_loop(0, width // WIDE, project, jnp.zeros((TOK, 1), F32))
    scale = lax.rsqrt(squares / width + EPSILON)
    rows[OWN] = (residual[...] * scale * feed_gain_ref[...]).astype(BF16)

    top, bottom = pl.ds(0, TOK // 2), pl.ds(TOK // 2, TOK // 2)
    near = [
        copy(rows.at[OWN, top], rows.at[LEFT, top], to_right),
        copy(rows.at[OWN, bottom], rows.at[RIGHT, bottom], to_left),
        copy(rows.at[OWN, bottom], rows.at[LEFT, bottom], to_right),
        copy(rows.at[OWN, top], rows.at[RIGHT, top], to_left),
    ]
    for move in near:
        move.start()
    relay = [
        copy(rows.at[LEFT, top], rows.at[FAR, top], to_right),
        copy(rows.at[RIGHT, bottom], rows.at[FAR, bottom], to_left),
    ]
    pump(PUMPS[8])
    for move, onward in zip(near, relay):
        move.wait_recv()
        onward.start()
    pump(64)
    gather.finish()
    near[2].wait_recv()
    near[3].wait_recv()
    for move in relay:
        move.wait()
    for move in near + head_near + head_far[:]:
        move.wait_send()

    def gate_up(cols):
        count = cols.size
        block = rows[...].reshape(4 * TOK, width)
        gate = whole[:, :, 0:32, cols].reshape(width, count)
        up = whole[:, :, 64:96, cols].reshape(width, count)
        gate = jnp.dot(block, gate, preferred_element_type=F32)
        up = jnp.dot(block, up, preferred_element_type=F32)
        hidden[:, cols] = (silu(gate) * up).astype(BF16)

    def gate_up_step(n, carry):
        gate_up(pl.ds(pl.multiple_of(n * WIDE, WIDE), WIDE))
        return carry

    units = hidden.shape[1]
    lax.fori_loop(0, units // WIDE, gate_up_step, 0)
    if units % WIDE:
        gate_up(pl.ds(units - units % WIDE, units % WIDE))

    def down(first, count, store):
        def step(n, carry):
            cols = pl.ds(pl.multiple_of(n * WIDE, WIDE), WIDE)
            matrix = whole[pl.ds(n * 4, 4), :, 32:64, :].reshape(WIDE, units)
            store(cols, mm_nt(hidden[first * TOK : (first + count) * TOK], matrix))
            return carry

        lax.fori_loop(0, width // WIDE, step, 0)

    def store_far(cols, tile):
        far_out[:, cols] = tile.astype(BF16)

    def store_near(cols, tile):
        outgoing[:, :, cols] = tile.astype(BF16).reshape(2, TOK, WIDE)

    def store_own(cols, tile):
        residual[:, cols] = residual[:, cols] + tile

    down(FAR, 1, store_far)
    far = [
        copy(far_out.at[top], relayed.at[0], to_right),
        copy(far_out.at[bottom], relayed.at[1], to_left),
    ]
    for move in far:
        move.start()
    down(RIGHT, 2, store_near)
    direct = [
        copy(outgoing.at[0, bottom], incoming.at[0, bottom], to_right),
        copy(outgoing.at[1, top], incoming.at[1, top], to_left),
    ]
    for move in direct:
        move.start()
    for move in far:
        move.wait_recv()
    outgoing[0, top] = (outgoing[0, top].astype(F32) + relayed[0].astype(F32)).astype(BF16)
    outgoing[1, bottom] = (outgoing[1, bottom].astype(F32) + relayed[1].astype(F32)).astype(BF16)
    combined = [
        copy(outgoing.at[0, top], incoming.at[0, top], to_right),
        copy(outgoing.at[1, bottom], incoming.at[1, bottom], to_left),
    ]
    for move in combined:
        move.start()
    down(OWN, 1, store_own)
    for move in direct + combined:
        move.wait()
    for move in far:
        move.wait_send()
    result_ref[...] = (
        residual[...] + (incoming[0].astype(F32) + incoming[1].astype(F32))
    ).astype(BF16)


PUMPS = (1, 2, 2, 1, 3, 3, 4, 2, 2)


def body(
    stream,
    query_projected,
    key_projected,
    value_projected,
    gate_projected,
    strength_logits,
    decay_preactivation,
    extra_log_decay,
    head_decay_rate,
    head_norm_gain,
    head_output_matrix,
    feed_norm_gain,
    gate_matrix,
    up_matrix,
    down_matrix,
):
    width = stream.shape[1]
    units = gate_matrix.shape[1]
    shard = jnp.concatenate([gate_matrix, down_matrix.T, up_matrix], axis=0)
    vmem = pl.BlockSpec(memory_space=pltpu.VMEM)
    pair = (HEAD, 2 * HEAD)
    square = (HEAD, HEAD)
    return pl.pallas_call(
        layer_kernel,
        name="layer",
        out_shape=jax.ShapeDtypeStruct(stream.shape, BF16),
        in_specs=[vmem] * 13,
        out_specs=vmem,
        scratch_shapes=[
            pltpu.VMEM((6, *pair), F32),
            pltpu.VMEM((6, *square), BF16),
            pltpu.VMEM((6, *square), F32),
            pltpu.VMEM((2, *pair), F32),
            pltpu.VMEM((2, *pair), BF16),
            pltpu.VMEM(pair, BF16),
            pltpu.VMEM((4, *pair), BF16),
            pltpu.VMEM(pair, BF16),
            pltpu.VMEM(pair, BF16),
            pltpu.VMEM(square, BF16),
            pltpu.VMEM(pair, BF16),
            pltpu.VMEM(pair, BF16),
            pltpu.VMEM(square, BF16),
            pltpu.VMEM(square, BF16),
            pltpu.VMEM(square, BF16),
            pltpu.VMEM((4 * TOK, 2 * HEAD), BF16),
            pltpu.VMEM((4, TOK, 2 * HEAD), BF16),
            pltpu.VMEM((4, 2, HEAD, width), BF16),
            pltpu.VMEM((TOK, width), F32),
            pltpu.VMEM((4, TOK, width), BF16),
            pltpu.VMEM((4 * TOK, units), BF16),
            pltpu.VMEM((32, 2, 96, units), BF16),
            pltpu.VMEM((TOK, width), BF16),
            pltpu.VMEM((2, TOK // 2, width), BF16),
            pltpu.VMEM((2, TOK, width), BF16),
            pltpu.VMEM((2, TOK, width), BF16),
            pltpu.SemaphoreType.DMA((40,)),
            pltpu.SemaphoreType.DMA((40,)),
            pltpu.SemaphoreType.DMA,
            pltpu.SemaphoreType.DMA,
            pltpu.SemaphoreType.DMA((96,)),
            pltpu.SemaphoreType.DMA,
        ],
        compiler_params=pltpu.CompilerParams(
            collective_id=0, has_side_effects=True, vmem_limit_bytes=60 * 1024 * 1024
        ),
    )(
        query_projected,
        key_projected,
        value_projected,
        gate_projected,
        strength_logits,
        decay_preactivation,
        extra_log_decay,
        head_decay_rate[:, None],
        head_norm_gain[None, :],
        stream,
        head_output_matrix,
        feed_norm_gain[None, :],
        shard,
    )


def solution(mesh):
    torus = Mesh(mesh.devices.reshape(8, 4, 2, mesh.shape["tp"]), ("sp_0", "sp_1", "sp_2", "tp"))
    in_specs = (
        P(SP_TP, None),
        P(SP, "tp"),
        P(SP, "tp"),
        P(SP, "tp"),
        P(SP, "tp"),
        P("tp", SP),
        P("tp", SP),
        P("tp", SP),
        P("tp"),
        P(),
        P("tp", None),
        P(),
        P(SP, "tp"),
        P(SP, "tp"),
        P("tp", SP),
    )
    out_specs = P(SP_TP, None)
    return jax.shard_map(body, mesh=torus, in_specs=in_specs, out_specs=out_specs, check_vma=False)
```

```python
import functools
import jax
import jax.numpy as jnp
from jax import lax
from jax.experimental import pallas as pl
from jax.experimental.pallas import tpu as pltpu
from jax.sharding import Mesh
from jax.sharding import PartitionSpec as P

HEAD = 128
CHUNK = 128
SP = ("sp_0", "sp_1", "sp_2")
SP_TP = ("sp_0", "sp_1", "sp_2", "tp")
EPSILON = 1e-06
F32 = jnp.float32
BF16 = jnp.bfloat16
HIGH = lax.Precision.HIGHEST
MESH = pl.DeviceIdType.MESH


def mm(a, b):
    return jnp.dot(a.astype(BF16), b.astype(BF16), preferred_element_type=F32)


def mm_nt(a, b):
    return lax.dot_general(a, b, (((1,), (1,)), ((), ())), preferred_element_type=F32)


def mm_tn(a, b):
    return lax.dot_general(
        a.astype(BF16), b.astype(BF16), (((0,), (0,)), ((), ())), preferred_element_type=F32
    )


def full(a, b):
    return jnp.dot(a, b, precision=HIGH, preferred_element_type=F32)


def full_nt(a, b):
    return lax.dot_general(
        a, b, (((1,), (1,)), ((), ())), precision=HIGH, preferred_element_type=F32
    )


def silu(x):
    return x / (1.0 + jnp.exp(-x))


def softplus(x):
    return jnp.maximum(x, 0.0) + jnp.log1p(jnp.exp(-jnp.abs(x)))


def halved(a):
    high = a.astype(BF16)
    return high, (a - high.astype(F32)).astype(BF16)


def precise(a, b):
    (ah, al), (bh, bl) = halved(a), halved(b)
    return jnp.dot(
        jnp.concatenate([ah, ah, al], axis=1),
        jnp.concatenate([bh, bl, bh], axis=0),
        preferred_element_type=F32,
    )


def local_part(
    q_ref, k_ref, v_ref, strength_ref, decay_ref, extra_ref, rate_ref, maps, from_state, from_values, pump
):
    row = lax.broadcasted_iota(jnp.int32, (CHUNK, CHUNK), 0)
    col = lax.broadcasted_iota(jnp.int32, (CHUNK, CHUNK), 1)
    eye = jnp.where(row == col, 1.0, 0.0)
    lower_ones = jnp.where(row >= col, 1.0, 0.0)
    upper_ones = jnp.where(row <= col, 1.0, 0.0)
    head = lax.broadcasted_iota(jnp.int32, (2, 1), 0)
    rate = jnp.where(head == 0, rate_ref[0], rate_ref[1])
    logs = -rate * softplus(decay_ref[...].astype(F32)) + extra_ref[...]
    beta = 1.0 / (1.0 + jnp.exp(-strength_ref[...].astype(F32)))
    padding = jnp.zeros((2, CHUNK), F32)
    spans = [slice(n * CHUNK, (n + 1) * CHUNK) for n in range(3)]
    logs = jnp.concatenate([logs[:, s] for s in spans] + [padding], axis=0)
    beta = jnp.concatenate([beta[:, s] for s in spans] + [padding], axis=0)
    sums_row = full(logs, upper_ones)
    sums_col = full_nt(lower_ones, logs)
    beta_col = full_nt(eye, beta)
    lowers, columns = [], []
    for u in range(6):
        span, cols = spans[u // 2], slice((u % 2) * HEAD, (u % 2 + 1) * HEAD)
        k, q = k_ref[span, cols], q_ref[span, cols]
        kf, qf = k.astype(F32), q.astype(F32)
        squares = kf * kf
        k_col = lax.rsqrt(jnp.sum(squares, axis=1, keepdims=True) + EPSILON)
        k_row = lax.rsqrt(full_nt(jnp.ones((8, HEAD), F32), squares)[0:1] + EPSILON)
        q_col = lax.rsqrt(jnp.sum(qf * qf, axis=1, keepdims=True) + EPSILON) * HEAD ** (-0.5)
        s_col, s_row, b_col = sums_col[:, u : u + 1], sums_row[u : u + 1], beta_col[:, u : u + 1]
        damping = jnp.exp(jnp.minimum(s_col - s_row, 0.0)) * k_row
        lowers.append(jnp.where(row > col, mm_nt(k, k) * damping * (b_col * k_col), 0.0))
        from_values[u] = jnp.where(row >= col, mm_nt(q, k) * damping * q_col, 0.0)
        columns.append((k_col, q_col, s_col, b_col, s_row[:, CHUNK - 1 :]))
    pump()
    nears = [jnp.where((row >> 3) == (col >> 3), lower, 0.0) for lower in lowers]
    inverses = [eye - near for near in nears]
    squares = [precise(d, d) for d in nears]
    inverses = [x + precise(x, s) for x, s in zip(inverses, squares)]
    squares = [precise(s, s) for s in squares]
    inverses = [x + precise(x, s) for x, s in zip(inverses, squares)]
    pump()
    for level in (3, 4, 5, 6):
        between = ((row >> (level + 1)) == (col >> (level + 1))) & ((row >> level) != (col >> level))
        parts = [jnp.where(between, lower, 0.0) for lower in lowers]
        parts = [precise(p, x) for p, x in zip(parts, inverses)]
        inverses = [x - precise(x, p) for p, x in zip(parts, inverses)]
        if level in (4, 6):
            pump()
    for u, (k_col, q_col, s_col, b_col, closing) in enumerate(columns):
        span, cols = spans[u // 2], slice((u % 2) * HEAD, (u % 2 + 1) * HEAD)
        kf, qf, vf = (r[span, cols].astype(F32) for r in (k_ref, q_ref, v_ref))
        opening = jnp.exp(s_col)
        right = jnp.concatenate([kf * (b_col * k_col * opening), vf * b_col], axis=1)
        solved = right + mm(inverses[u] - eye, right)
        change = mm_tn(kf * (k_col * jnp.exp(closing - s_col)), solved)
        maps[u, :, :HEAD] = (jnp.exp(closing) - 1.0) * eye - change[:, :HEAD]
        maps[u, :, HEAD:] = change[:, HEAD:]
        out = mm(from_values[u], solved)
        from_state[u] = (qf * (q_col * opening) - out[:, :HEAD]).astype(BF16)
        from_values[u] = out[:, HEAD:]
    pump()


def joined(earlier, later):
    return earlier + later + mm(later[:, :HEAD], earlier)


def carried(state, pair):
    return state + pair[:, HEAD:] + mm(pair[:, :HEAD], state)


GATE_ROWS = (0, 32)
DOWN_ROWS = (32, 32)
UP_ROWS = (64, 32)


def halves(rows):
    first, count = rows
    return (first, count // 2), (first + count // 2, count // 2)


def sides(rows, offsets, place):
    if len(offsets) == 2:
        return [(place(offsets[0]), rows)], [(place(offsets[1]), rows)]
    low, high = halves(rows)
    return [(place(offsets[0]), low)], [(place(offsets[0]), high)]


class Gather:
    def __init__(self, z, y, c, shard, whole, sems):
        self.z, self.y, self.c, self.shard, self.whole = z, y, c, shard, whole
        self.ring_send, self.sib_send, self.ring_recv, self.sib_recv = sems
        self.used = 0
        self.moves = {}
        self.columns = [(0,), (-1, 1), (-2, 2), (-3, 3), (-4,)]
        self.lines = [(0,), (-1, 1), (2,)]
        for flow, rows in (("g", GATE_ROWS), ("d", DOWN_ROWS)):
            for s in (1, 2, 3):
                for way in (1, -1):
                    self.plan(flow + "z", s, way, 0, [((-way * s, 0), rows)])
            for way, blocks in zip((1, -1), sides(rows, (-4,), lambda o: (o, 0))):
                self.plan(flow + "z", 4, way, 0, blocks)
            for n, offsets in enumerate(self.columns):
                for way in (1, -1):
                    self.plan(flow + "y", (n, 1), way, 1, [((o, -way), rows) for o in offsets])
                for way, blocks in zip((1, -1), sides(rows, offsets, lambda o: (o, 2))):
                    self.plan(flow + "y", (n, 2), way, 1, blocks)
        for way in (1, -1):
            self.plan("uy", 1, way, 1, [((0, -way), UP_ROWS)])
        for way, blocks in zip((1, -1), sides(UP_ROWS, (2,), lambda o: (0, o))):
            self.plan("uy", 2, way, 1, blocks)
        for n, offsets in enumerate(self.lines):
            for s in (1, 2, 3):
                for way in (1, -1):
                    self.plan("uz", (n, s), way, 0, [((-way * s, o), UP_ROWS) for o in offsets])
            for way, blocks in zip((1, -1), sides(UP_ROWS, offsets, lambda o: (4, o))):
                self.plan("uz", (n, 4), way, 0, blocks)

    def plan(self, flow, step, way, axis, blocks):
        entries = []
        for place, rows in blocks:
            entries.append((place, rows, self.used))
            self.used += 1
        self.moves[flow, step, way] = (axis, entries)

    def block(self, place, rows):
        z = (self.z + place[0] + 8) % 8
        y = (self.y + place[1] + 8) % 4
        return self.whole.at[z * 4 + y, self.c, pl.ds(*rows)]

    def copy(self, axis, way, place, rows, sem, src, dst):
        name, size, at = (("sp_0", 8, self.z), ("sp_1", 4, self.y))[axis]
        return pltpu.make_async_remote_copy(
            src_ref=src,
            dst_ref=dst,
            send_sem=self.ring_send,
            recv_sem=self.ring_recv.at[sem],
            device_id={name: (at + way + size) % size},
            device_id_type=MESH,
        )

    def send(self, flow, step):
        for way in (1, -1):
            axis, entries = self.moves[flow, step, way]
            for place, rows, sem in entries:
                shift = (place[0] + way, place[1]) if axis == 0 else (place[0], place[1] + way)
                dst = self.block(shift, rows)
                own = shift[0] % 8 == 0 and shift[1] % 4 == 0
                src = self.shard.at[pl.ds(*rows)] if own else dst
                self.copy(axis, way, place, rows, sem, src, dst).start()

    def receive(self, flow, step):
        for way in (1, -1):
            axis, entries = self.moves[flow, step, way]
            for place, rows, sem in entries:
                block = self.block(place, rows)
                self.copy(axis, way, place, rows, sem, block, block).wait_recv()
                self.across(block, block, rows[0] // 32).start()

    def across(self, src, dst, part):
        return pltpu.make_async_remote_copy(
            src_ref=src,
            dst_ref=dst,
            send_sem=self.sib_send,
            recv_sem=self.sib_recv.at[part],
            device_id={"sp_2": 1 - self.c},
            device_id_type=MESH,
        )

    def start(self):
        self.send("uy", 1)
        self.send("gz", 1)
        self.send("gy", (0, 1))
        self.send("uz", (0, 1))
        self.send("dz", 1)
        here = self.z * 4 + self.y
        for part in range(3):
            rows = pl.ds(32 * part, 32)
            self.across(self.shard.at[rows], self.whole.at[here, self.c, rows], part).start()
        self.whole[here, self.c] = self.shard[...]

    def handle(self, kind, *step):
        if kind[1] == "s":
            self.send({"g": "gy", "d": "dy", "u": "uz"}[kind[0]], (step[0], 1))
            return
        self.receive(kind, step if len(step) > 1 else step[0])
        if kind in ("gz", "dz"):
            if step[0] < 4:
                self.send(kind, step[0] + 1)
        elif kind in ("gy", "dy"):
            if step[1] == 1:
                self.send(kind, (step[0], 2))
        elif kind == "uy":
            if step[0] == 1:
                self.send("uy", 2)
        elif step[1] < 4:
            self.send("uz", (step[0], step[1] + 1))

    def from_sibling(self, part):
        block = self.whole.at[:, 1 - self.c, pl.ds(32 * part, 32)]
        self.across(block, block, part).wait_recv()

    def finish(self):
        sibling = self.whole.at[:, 1 - self.c]
        self.across(sibling, sibling, 0).wait_send()
        most = self.whole.at[pl.ds(0, 31), self.c]
        self.copy(0, 1, None, None, 0, most, most).wait_send()


FAR, RIGHT, LEFT, OWN = range(4)
TOK = 96
WIDE = 256


def layer_kernel(
    q_ref,
    k_ref,
    v_ref,
    gate_ref,
    strength_ref,
    decay_ref,
    extra_ref,
    rate_ref,
    gain_ref,
    stream_ref,
    head_ref,
    feed_gain_ref,
    gate_shard,
    up_shard,
    down_shard,
    result_ref,
    maps,
    from_state,
    from_values,
    totals,
    pair,
    sib,
    chip,
    zin1,
    zin2,
    zin4,
    zout1,
    zout2,
    zout4,
    hin,
    hout,
    mixed,
    mixed_in,
    head_whole,
    residual,
    rows,
    hidden,
    shard,
    whole,
    far_out,
    relayed,
    outgoing,
    incoming,
    send_sem,
    recv_sem,
    ring_send,
    sib_send,
    ring_recv,
    sib_recv,
):
    z, y, c = lax.axis_index("sp_0"), lax.axis_index("sp_1"), lax.axis_index("sp_2")
    x = lax.axis_index("tp")
    for ref in (zin1, zin2, zin4):
        ref[...] = jnp.zeros_like(ref)
    to_sibling = {"sp_2": 1 - c}
    to_right, to_left, to_far = ({"tp": lax.rem(x + d, 4)} for d in (1, 3, 2))
    barrier = pltpu.get_barrier_semaphore()
    peers = [to_sibling, to_right, to_left, to_far]
    peers += [{"sp_1": lax.rem(y + d, 4)} for d in (1, 2, 3)]
    peers += [{"sp_0": lax.rem(z + d, 8)} for d in (1, 2, 4, 6, 7)]
    for peer in peers:
        pl.semaphore_signal(barrier, inc=1, device_id=peer, device_id_type=MESH)
    shard[0:32] = gate_shard[...]
    shard[32:64] = down_shard[...].astype(F32).T.astype(BF16)
    shard[64:96] = up_shard[...]
    pl.semaphore_wait(barrier, len(peers))

    gather = Gather(z, y, c, shard, whole, (ring_send, sib_send, ring_recv, sib_recv))
    gather.start()
    schedule = iter(SCHEDULE)

    def pump():
        for event in next(schedule):
            gather.handle(*event)

    slots = iter(range(64))

    def copy(src, dst, peer):
        slot = next(slots)
        return pltpu.make_async_remote_copy(
            src_ref=src,
            dst_ref=dst,
            send_sem=send_sem.at[slot],
            recv_sem=recv_sem.at[slot],
            device_id=peer,
            device_id_type=MESH,
        )

    half = head_ref.at[pl.ds(pl.multiple_of(c * HEAD, HEAD), HEAD)]
    head_near = [
        copy(half, head_whole.at[LEFT, c], to_right),
        copy(half, head_whole.at[RIGHT, c], to_left),
    ]
    for move in head_near:
        move.start()
    low, high = pl.ds(0, HEAD // 2), pl.ds(HEAD // 2, HEAD // 2)
    head_far = [
        copy(head_whole.at[LEFT, c, low], head_whole.at[FAR, c, low], to_right),
        copy(head_whole.at[RIGHT, c, high], head_whole.at[FAR, c, high], to_left),
    ]
    head_sib = [
        copy(head_whole.at[side, c], head_whole.at[side, c], to_sibling) for side in (FAR, RIGHT, LEFT)
    ]

    local_part(
        q_ref,
        k_ref,
        v_ref,
        strength_ref,
        decay_ref,
        extra_ref,
        rate_ref,
        maps,
        from_state,
        from_values,
        pump,
    )
    for h in range(2):
        total = joined(joined(maps[h], maps[2 + h]), maps[4 + h])
        totals[h] = total
        pair[h] = total.astype(BF16)

    to_sib = copy(pair.at[1 - c], sib, to_sibling)
    to_sib.start()
    pump()
    to_sib.wait()
    own, other = totals[c], sib[...].astype(F32)
    first = jnp.where(c == 0, own, other)
    chip[y] = joined(first, jnp.where(c == 0, other, own)).astype(BF16)
    totals[1] = first

    sends = []
    for d in (1, 2, 3):
        sends.append(copy(chip.at[y], chip.at[y], {"sp_1": lax.rem(y + d, 4)}))
        sends[-1].start()
    pump()
    for d in (1, 2, 3):
        sends[d - 1].wait()
    total = chip[0].astype(F32)
    before = jnp.where(y == 0, 0.0, total)
    for s in (1, 2, 3):
        total = joined(total, chip[s].astype(F32))
        if s < 3:
            before = jnp.where(y > s, total, before)

    totals[0] = before
    earlier = jnp.zeros((HEAD, 2 * HEAD), F32)
    for n, (d, out, arrived) in enumerate(((1, zout1, zin1), (2, zout2, zin2), (4, zout4, zin4))):
        out[...] = total[:, (2 * HEAD - out.shape[1]) :].astype(BF16)
        hop = copy(out, arrived, {"sp_0": lax.rem(z + d, 8)})

        @pl.when(z + d < 8)
        def _():
            hop.start()

        pump()

        @pl.when(z >= d)
        def _():
            hop.wait_recv()

        came = arrived[...].astype(F32)
        if d < 4:
            earlier = joined(came, earlier)
            total = joined(came, total)
        else:
            state = carried(came, earlier)

        @pl.when(z + d < 8)
        def _():
            hop.wait_send()

        if n == 0:
            for near, far in zip(head_near, head_far):
                near.wait_recv()
                far.start()
            head_sib[2].start()
            head_sib[1].start()
        if n == 2:
            for far in head_far:
                far.wait_recv()
            head_sib[0].start()

    state = carried(state, totals[0])
    later = carried(state, totals[1])
    hout[...] = jnp.where(c == 0, later, state).astype(BF16)
    across = copy(hout, hin, to_sibling)
    across.start()

    def outputs(h, state):
        cols = pl.ds(pl.multiple_of(h * HEAD, HEAD), HEAD)
        for n in range(3):
            u = n * 2 + h
            span = slice(n * CHUNK, (n + 1) * CHUNK)
            out = from_values[u] + mm(from_state[u], state)
            if n < 2:
                state = carried(state, maps[u])
            out = out * lax.rsqrt(jnp.mean(out * out, axis=1, keepdims=True) + EPSILON)
            gated = out * gain_ref[...] * silu(gate_ref[span, cols].astype(F32))
            mixed[span, cols] = gated.astype(BF16)

    outputs(c, jnp.where(c == 0, state, later))
    pump()
    across.wait()
    outputs(1 - c, hin[...].astype(F32))

    def rows_of(d):
        return pl.ds(pl.multiple_of(lax.rem(x + d, 4) * TOK, TOK), TOK)

    exchange = [
        copy(mixed.at[rows_of(2)], mixed_in.at[FAR], to_far),
        copy(mixed.at[rows_of(1)], mixed_in.at[LEFT], to_right),
        copy(mixed.at[rows_of(3)], mixed_in.at[RIGHT], to_left),
    ]
    for move in exchange:
        move.start()
    pump()
    mixed_in[OWN] = mixed[rows_of(0), :]
    for move in head_sib:
        move.wait()
    head_whole[OWN] = head_ref[...].reshape(2, HEAD, -1)
    for move in exchange:
        move.wait()

    width = residual.shape[1]
    block = jnp.concatenate([mixed_in[side] for side in range(4)], axis=1)
    squares = jnp.zeros((TOK, 1), F32)
    for first in range(0, width, 2 * WIDE):
        cols = slice(first, first + 2 * WIDE)
        matrix = head_whole[:, :, :, cols].reshape(8 * HEAD, 2 * WIDE)
        tile = jnp.dot(block, matrix, preferred_element_type=F32) + stream_ref[:, cols].astype(F32)
        residual[:, cols] = tile
        squares = squares + jnp.sum(tile * tile, axis=1, keepdims=True)
    pump()
    scale = lax.rsqrt(squares / width + EPSILON)
    rows[OWN] = (residual[...] * scale * feed_gain_ref[...]).astype(BF16)

    top, bottom = pl.ds(0, TOK // 2), pl.ds(TOK // 2, TOK // 2)
    near = [
        copy(rows.at[OWN, top], rows.at[LEFT, top], to_right),
        copy(rows.at[OWN, bottom], rows.at[RIGHT, bottom], to_left),
        copy(rows.at[OWN, bottom], rows.at[LEFT, bottom], to_right),
        copy(rows.at[OWN, top], rows.at[RIGHT, top], to_left),
    ]
    for move in near:
        move.start()
    relay = [
        copy(rows.at[LEFT, top], rows.at[FAR, top], to_right),
        copy(rows.at[RIGHT, bottom], rows.at[FAR, bottom], to_left),
    ]
    pump()
    for move, onward in zip(near, relay):
        move.wait_recv()
        onward.start()
    pump()
    gather.from_sibling(0)
    gather.from_sibling(2)
    near[2].wait_recv()
    near[3].wait_recv()

    def gate_up(first, count, cols):
        tile = cols.stop - cols.start
        block = rows[first : first + count].reshape(count * TOK, width)
        gate = whole[:, :, 0:32, cols].reshape(width, tile)
        up = whole[:, :, 64:96, cols].reshape(width, tile)
        gate = jnp.dot(block, gate, preferred_element_type=F32)
        up = jnp.dot(block, up, preferred_element_type=F32)
        hidden[first * TOK : (first + count) * TOK, cols] = (silu(gate) * up).astype(BF16)

    units = hidden.shape[1]
    tiles = [slice(n, min(n + WIDE, units)) for n in range(0, units, WIDE)]
    for cols in tiles:
        gate_up(RIGHT, 3, cols)
        pump()
    for move in relay:
        move.wait()
    for cols in tiles:
        gate_up(FAR, 1, cols)
    pump()
    gather.from_sibling(1)

    def down(first, count, store, part=(0, 2)):
        def step(n, carry):
            cols = pl.ds(pl.multiple_of(n * WIDE, WIDE), WIDE)
            matrix = whole[pl.ds(n * 4, 4), :, 32:64, :].reshape(WIDE, units)
            store(cols, mm_nt(hidden[first * TOK : (first + count) * TOK], matrix))
            return carry

        steps = width // WIDE // 2
        lax.fori_loop(part[0] * steps, part[1] * steps, step, 0)

    def store_far(cols, tile):
        far_out[:, cols] = tile.astype(BF16)

    def store_near(cols, tile):
        outgoing[:, :, cols] = tile.astype(BF16).reshape(2, TOK, WIDE)

    def store_own(cols, tile):
        residual[:, cols] = residual[:, cols] + tile

    far, direct, combined = [], [], []
    for part in range(2):
        cols = pl.ds(part * width // 2, width // 2)
        down(FAR, 1, store_far, (part, part + 1))
        far += [
            copy(far_out.at[top, cols], relayed.at[0, :, cols], to_right),
            copy(far_out.at[bottom, cols], relayed.at[1, :, cols], to_left),
        ]
        for move in far[-2:]:
            move.start()
    for part in range(2):
        cols = pl.ds(part * width // 2, width // 2)
        down(RIGHT, 2, store_near, (part, part + 1))
        direct += [
            copy(outgoing.at[0, bottom, cols], incoming.at[0, bottom, cols], to_right),
            copy(outgoing.at[1, top, cols], incoming.at[1, top, cols], to_left),
        ]
        for move in direct[-2:]:
            move.start()
    for part in range(2):
        cols = pl.ds(part * width // 2, width // 2)
        for side, rows_half in ((0, top), (1, bottom)):
            far[2 * part + side].wait_recv()
            mine = outgoing[side, rows_half, cols].astype(F32)
            outgoing[side, rows_half, cols] = (mine + relayed[side, :, cols].astype(F32)).astype(BF16)
        combined += [
            copy(outgoing.at[0, top, cols], incoming.at[0, top, cols], to_right),
            copy(outgoing.at[1, bottom, cols], incoming.at[1, bottom, cols], to_left),
        ]
        for move in combined[-2:]:
            move.start()
    down(OWN, 1, store_own)
    for move in direct + combined:
        move.wait()
    for move in far:
        move.wait_send()
    result_ref[...] = (
        residual[...] + (incoming[0].astype(F32) + incoming[1].astype(F32))
    ).astype(BF16)
    for move in near + head_near + head_far:
        move.wait_send()
    gather.finish()


SCHEDULE = (
    (("ds", 0),),
    (),
    (),
    (),
    (("uy", 1), ("gz", 1),),
    (("gy", 0, 1), ("uz", 0, 1),),
    (("gs", 1), ("us", 1), ("uy", 2), ("dy", 0, 1), ("gz", 2), ("gs", 2), ("gy", 0, 2),),
    (("dz", 1), ("gz", 3), ("gs", 3), ("gy", 1, 1),),
    (("us", 2), ("uz", 0, 2), ("gz", 4), ("gs", 4), ("gy", 2, 1), ("dy", 0, 2),),
    (("uz", 1, 1), ("uz", 2, 1), ("dz", 2), ("ds", 1), ("gy", 1, 2),),
    (("uz", 0, 3), ("gy", 3, 1),),
    (("gy", 2, 2), ("ds", 2), ("dz", 3), ("uz", 1, 2), ("uz", 2, 2),),
    (("uz", 0, 4), ("ds", 3), ("gy", 4, 1), ("gy", 3, 2),),
    (("dz", 4), ("ds", 4), ("uz", 1, 3), ("uz", 2, 3), ("dy", 1, 1),),
    (("dy", 2, 1), ("dy", 3, 1), ("uz", 1, 4), ("uz", 2, 4), ("gy", 4, 2), ("dy", 4, 1),),
    (),
    (),
    (("dy", 1, 2),),
    (),
    (("dy", 2, 2),),
    (("dy", 3, 2),),
    (("dy", 4, 2),),
)


def body(
    stream,
    query_projected,
    key_projected,
    value_projected,
    gate_projected,
    strength_logits,
    decay_preactivation,
    extra_log_decay,
    head_decay_rate,
    head_norm_gain,
    head_output_matrix,
    feed_norm_gain,
    gate_matrix,
    up_matrix,
    down_matrix,
):
    width = stream.shape[1]
    units = gate_matrix.shape[1]
    vmem = pl.BlockSpec(memory_space=pltpu.VMEM)
    pair = (HEAD, 2 * HEAD)
    square = (HEAD, HEAD)
    return pl.pallas_call(
        layer_kernel,
        name="layer",
        out_shape=jax.ShapeDtypeStruct(stream.shape, BF16),
        in_specs=[vmem] * 7 + [pl.BlockSpec(memory_space=pltpu.SMEM)] + [vmem] * 7,
        out_specs=vmem,
        scratch_shapes=[
            pltpu.VMEM((6, *pair), F32),
            pltpu.VMEM((6, *square), BF16),
            pltpu.VMEM((6, *square), F32),
            pltpu.VMEM((2, *pair), F32),
            pltpu.VMEM((2, *pair), BF16),
            pltpu.VMEM(pair, BF16),
            pltpu.VMEM((4, *pair), BF16),
            pltpu.VMEM(pair, BF16),
            pltpu.VMEM(pair, BF16),
            pltpu.VMEM(square, BF16),
            pltpu.VMEM(pair, BF16),
            pltpu.VMEM(pair, BF16),
            pltpu.VMEM(square, BF16),
            pltpu.VMEM(square, BF16),
            pltpu.VMEM(square, BF16),
            pltpu.VMEM((4 * TOK, 2 * HEAD), BF16),
            pltpu.VMEM((4, TOK, 2 * HEAD), BF16),
            pltpu.VMEM((4, 2, HEAD, width), BF16),
            pltpu.VMEM((TOK, width), F32),
            pltpu.VMEM((4, TOK, width), BF16),
            pltpu.VMEM((4 * TOK, units), BF16),
            pltpu.VMEM((96, units), BF16),
            pltpu.VMEM((32, 2, 96, units), BF16),
            pltpu.VMEM((TOK, width), BF16),
            pltpu.VMEM((2, TOK // 2, width), BF16),
            pltpu.VMEM((2, TOK, width), BF16),
            pltpu.VMEM((2, TOK, width), BF16),
            pltpu.SemaphoreType.DMA((48,)),
            pltpu.SemaphoreType.DMA((48,)),
            pltpu.SemaphoreType.DMA,
            pltpu.SemaphoreType.DMA,
            pltpu.SemaphoreType.DMA((104,)),
            pltpu.SemaphoreType.DMA((3,)),
        ],
        compiler_params=pltpu.CompilerParams(
            collective_id=0, has_side_effects=True, vmem_limit_bytes=60 * 1024 * 1024
        ),
    )(
        query_projected,
        key_projected,
        value_projected,
        gate_projected,
        strength_logits,
        decay_preactivation,
        extra_log_decay,
        head_decay_rate,
        head_norm_gain[None, :],
        stream,
        head_output_matrix,
        feed_norm_gain[None, :],
        gate_matrix,
        up_matrix,
        down_matrix,
    )


def solution(mesh):
    torus = Mesh(mesh.devices.reshape(8, 4, 2, mesh.shape["tp"]), ("sp_0", "sp_1", "sp_2", "tp"))
    in_specs = (
        P(SP_TP, None),
        P(SP, "tp"),
        P(SP, "tp"),
        P(SP, "tp"),
        P(SP, "tp"),
        P("tp", SP),
        P("tp", SP),
        P("tp", SP),
        P("tp"),
        P(),
        P("tp", None),
        P(),
        P(SP, "tp"),
        P(SP, "tp"),
        P("tp", SP),
    )
    out_specs = P(SP_TP, None)
    return jax.shard_map(body, mesh=torus, in_specs=in_specs, out_specs=out_specs, check_vma=False)
```

```python
import functools
import jax
import jax.numpy as jnp
from jax import lax
from jax.experimental import pallas as pl
from jax.experimental.pallas import tpu as pltpu
from jax.sharding import Mesh
from jax.sharding import PartitionSpec as P

HEAD = 128
CHUNK = 128
SP = ("sp_0", "sp_1", "sp_2")
SP_TP = ("sp_0", "sp_1", "sp_2", "tp")
EPSILON = 1e-06
F32 = jnp.float32
BF16 = jnp.bfloat16
HIGH = lax.Precision.HIGHEST
MESH = pl.DeviceIdType.MESH


def mm(a, b):
    return jnp.dot(a.astype(BF16), b.astype(BF16), preferred_element_type=F32)


def mm_nt(a, b):
    return lax.dot_general(a, b, (((1,), (1,)), ((), ())), preferred_element_type=F32)


def mm_tn(a, b):
    return lax.dot_general(
        a.astype(BF16), b.astype(BF16), (((0,), (0,)), ((), ())), preferred_element_type=F32
    )


def full(a, b):
    return jnp.dot(a, b, precision=HIGH, preferred_element_type=F32)


def full_nt(a, b):
    return lax.dot_general(
        a, b, (((1,), (1,)), ((), ())), precision=HIGH, preferred_element_type=F32
    )


def silu(x):
    return x / (1.0 + jnp.exp(-x))


def softplus(x):
    return jnp.maximum(x, 0.0) + jnp.log1p(jnp.exp(-jnp.abs(x)))


def halved(a):
    high = a.astype(BF16)
    return high, (a - high.astype(F32)).astype(BF16)


def precise(a, b):
    (ah, al), (bh, bl) = halved(a), halved(b)
    return jnp.dot(
        jnp.concatenate([ah, ah, al], axis=1),
        jnp.concatenate([bh, bl, bh], axis=0),
        preferred_element_type=F32,
    )


def local_part(
    q_ref, k_ref, v_ref, strength_ref, decay_ref, extra_ref, rate_ref, maps, from_state, from_values, begin, pump
):
    row = lax.broadcasted_iota(jnp.int32, (CHUNK, CHUNK), 0)
    col = lax.broadcasted_iota(jnp.int32, (CHUNK, CHUNK), 1)
    eye = jnp.where(row == col, 1.0, 0.0)
    lower_ones = jnp.where(row >= col, 1.0, 0.0)
    upper_ones = jnp.where(row <= col, 1.0, 0.0)
    head = lax.broadcasted_iota(jnp.int32, (2, 1), 0)
    rate = jnp.where(head == 0, rate_ref[0], rate_ref[1])
    logs = -rate * softplus(decay_ref[...].astype(F32)) + extra_ref[...]
    beta = 1.0 / (1.0 + jnp.exp(-strength_ref[...].astype(F32)))
    padding = jnp.zeros((2, CHUNK), F32)
    spans = [slice(n * CHUNK, (n + 1) * CHUNK) for n in range(3)]
    logs = jnp.concatenate([logs[:, s] for s in spans] + [padding], axis=0)
    beta = jnp.concatenate([beta[:, s] for s in spans] + [padding], axis=0)
    sums_row = full(logs, upper_ones)
    sums_col = full_nt(lower_ones, logs)
    beta_col = full_nt(eye, beta)
    lowers, columns = [], []
    for u in range(6):
        span, cols = spans[u // 2], slice((u % 2) * HEAD, (u % 2 + 1) * HEAD)
        k, q = k_ref[span, cols], q_ref[span, cols]
        kf, qf = k.astype(F32), q.astype(F32)
        squares = kf * kf
        k_col = lax.rsqrt(jnp.sum(squares, axis=1, keepdims=True) + EPSILON)
        k_row = lax.rsqrt(full_nt(jnp.ones((8, HEAD), F32), squares)[0:1] + EPSILON)
        q_col = lax.rsqrt(jnp.sum(qf * qf, axis=1, keepdims=True) + EPSILON) * HEAD ** (-0.5)
        s_col, s_row, b_col = sums_col[:, u : u + 1], sums_row[u : u + 1], beta_col[:, u : u + 1]
        damping = jnp.exp(jnp.minimum(s_col - s_row, 0.0)) * k_row
        lowers.append(jnp.where(row > col, mm_nt(k, k) * damping * (b_col * k_col), 0.0))
        from_values[u] = jnp.where(row >= col, mm_nt(q, k) * damping * q_col, 0.0)
        columns.append((k_col, q_col, s_col, b_col, s_row[:, CHUNK - 1 :]))
    begin()
    pump()
    nears = [jnp.where((row >> 3) == (col >> 3), lower, 0.0) for lower in lowers]
    inverses = [eye - near for near in nears]
    squares = [precise(d, d) for d in nears]
    inverses = [x + precise(x, s) for x, s in zip(inverses, squares)]
    squares = [precise(s, s) for s in squares]
    inverses = [x + precise(x, s) for x, s in zip(inverses, squares)]
    pump()
    for level in (3, 4, 5, 6):
        between = ((row >> (level + 1)) == (col >> (level + 1))) & ((row >> level) != (col >> level))
        parts = [jnp.where(between, lower, 0.0) for lower in lowers]
        parts = [precise(p, x) for p, x in zip(parts, inverses)]
        inverses = [x - precise(x, p) for p, x in zip(parts, inverses)]
        if level in (4, 6):
            pump()
    for u, (k_col, q_col, s_col, b_col, closing) in enumerate(columns):
        span, cols = spans[u // 2], slice((u % 2) * HEAD, (u % 2 + 1) * HEAD)
        kf, qf, vf = (r[span, cols].astype(F32) for r in (k_ref, q_ref, v_ref))
        opening = jnp.exp(s_col)
        right = jnp.concatenate([kf * (b_col * k_col * opening), vf * b_col], axis=1)
        solved = right + mm(inverses[u] - eye, right)
        change = mm_tn(kf * (k_col * jnp.exp(closing - s_col)), solved)
        maps[u, :, :HEAD] = (jnp.exp(closing) - 1.0) * eye - change[:, :HEAD]
        maps[u, :, HEAD:] = change[:, HEAD:]
        out = mm(from_values[u], solved)
        from_state[u] = (qf * (q_col * opening) - out[:, :HEAD]).astype(BF16)
        from_values[u] = out[:, HEAD:]
    pump()


def joined(earlier, later):
    return earlier + later + mm(later[:, :HEAD], earlier)


def carried(state, pair):
    return state + pair[:, HEAD:] + mm(pair[:, :HEAD], state)


def halves(region):
    first, count = region
    return (first, count // 2), (first + count // 2, count // 2)


def sides(rows, offsets, place):
    if len(offsets) == 2:
        return [(place(offsets[0]), rows)], [(place(offsets[1]), rows)]
    low, high = halves(rows)
    return [(place(offsets[0]), low)], [(place(offsets[0]), high)]


class Gather:
    def __init__(self, z, y, c, shard, whole, sems):
        self.z, self.y, self.c, self.shard, self.whole = z, y, c, shard, whole
        self.ring_send, self.sib_send, self.ring_recv, self.sib_recv = sems
        self.used = 0
        self.moves = {}
        self.columns = [(0,), (-1, 1), (-2, 2), (-3, 3), (-4,)]
        self.lines = [(0,), (-1,), (1,), (2,)]
        gate, down, up = (0, 32), (32, 32), (64, 32)
        for flow, rows in (("g", gate), ("d", down)):
            for s in (1, 2, 3):
                for way in (1, -1):
                    self.plan(flow + "z", s, way, 0, [((-way * s, 0), rows)])
            for way, blocks in zip((1, -1), sides(rows, (-4,), lambda o: (o, 0))):
                self.plan(flow + "z", 4, way, 0, blocks)
            for n, offsets in enumerate(self.columns):
                for way in (1, -1):
                    self.plan(flow + "y", (n, 1), way, 1, [((o, -way), rows) for o in offsets])
                for way, blocks in zip((1, -1), sides(rows, offsets, lambda o: (o, 2))):
                    self.plan(flow + "y", (n, 2), way, 1, blocks)
        for flow, rows in (("u", up),):
            for way in (1, -1):
                self.plan(flow + "y", 1, way, 1, [((0, -way), rows)])
            for way, blocks in zip((1, -1), sides(rows, (2,), lambda o: (0, o))):
                self.plan(flow + "y", 2, way, 1, blocks)
            for n, offsets in enumerate(self.lines):
                for s in (1, 2, 3):
                    for way in (1, -1):
                        self.plan(flow + "z", (n, s), way, 0, [((-way * s, o), rows) for o in offsets])
                for way, blocks in zip((1, -1), sides(rows, offsets, lambda o: (4, o))):
                    self.plan(flow + "z", (n, 4), way, 0, blocks)

    def plan(self, flow, step, way, axis, blocks):
        entries = []
        for place, rows in blocks:
            entries.append((place, rows, self.used))
            self.used += 1
        self.moves[flow, step, way] = (axis, entries)

    def block(self, place, rows):
        z = (self.z + place[0] + 8) % 8
        y = (self.y + place[1] + 8) % 4
        return self.whole.at[z * 4 + y, self.c, pl.ds(*rows)]

    def copy(self, axis, way, place, rows, sem, src, dst):
        name, size, at = (("sp_0", 8, self.z), ("sp_1", 4, self.y))[axis]
        return pltpu.make_async_remote_copy(
            src_ref=src,
            dst_ref=dst,
            send_sem=self.ring_send,
            recv_sem=self.ring_recv.at[sem],
            device_id={name: (at + way + size) % size},
            device_id_type=MESH,
        )

    def send(self, flow, step):
        for way in (1, -1):
            axis, entries = self.moves[flow, step, way]
            for place, rows, sem in entries:
                shift = (place[0] + way, place[1]) if axis == 0 else (place[0], place[1] + way)
                dst = self.block(shift, rows)
                own = shift[0] % 8 == 0 and shift[1] % 4 == 0
                src = self.shard.at[pl.ds(*rows)] if own else dst
                self.copy(axis, way, place, rows, sem, src, dst).start()

    def receive(self, flow, step):
        for way in (1, -1):
            axis, entries = self.moves[flow, step, way]
            for place, rows, sem in entries:
                block = self.block(place, rows)
                self.copy(axis, way, place, rows, sem, block, block).wait_recv()
                self.across(block, block, rows[0] // 32).start()

    def across(self, src, dst, part):
        return pltpu.make_async_remote_copy(
            src_ref=src,
            dst_ref=dst,
            send_sem=self.sib_send,
            recv_sem=self.sib_recv.at[part],
            device_id={"sp_2": 1 - self.c},
            device_id_type=MESH,
        )

    def start(self):
        self.send("uy", 1)
        self.send("gz", 1)
        self.send("gy", (0, 1))
        self.send("uz", (0, 1))
        self.send("dz", 1)
        here = self.z * 4 + self.y
        for part in range(3):
            rows = pl.ds(32 * part, 32)
            self.across(self.shard.at[rows], self.whole.at[here, self.c, rows], part).start()
        self.whole[here, self.c] = self.shard[...]

    def handle(self, kind, *step):
        if kind[1] == "s":
            self.send({"g": "gy", "d": "dy", "u": "uz"}[kind[0]], (step[0], 1))
            return
        self.receive(kind, step if len(step) > 1 else step[0])
        if kind in ("gz", "dz"):
            if step[0] < 4:
                self.send(kind, step[0] + 1)
        elif kind in ("gy", "dy"):
            if step[1] == 1:
                self.send(kind, (step[0], 2))
        elif kind == "uy":
            if step[0] == 1:
                self.send(kind, 2)
        elif step[1] < 4:
            self.send(kind, (step[0], step[1] + 1))

    def from_sibling(self, part):
        block = self.whole.at[:, 1 - self.c, pl.ds(32 * part, 32)]
        self.across(block, block, part).wait_recv()

    def finish(self):
        sibling = self.whole.at[:, 1 - self.c]
        self.across(sibling, sibling, 0).wait_send()
        most = self.whole.at[pl.ds(0, 31), self.c]
        self.copy(0, 1, None, None, 0, most, most).wait_send()


FAR, RIGHT, LEFT, OWN = range(4)
TOK = 96
WIDE = 256


def layer_kernel(
    q_hbm,
    k_hbm,
    v_hbm,
    gate_hbm,
    strength_hbm,
    decay_hbm,
    extra_hbm,
    rate_ref,
    gain_ref,
    stream_hbm,
    head_hbm,
    feed_gain_ref,
    gate_shard,
    up_shard,
    down_shard,
    result_ref,
    q_ref,
    k_ref,
    v_ref,
    gate_ref,
    strength_ref,
    decay_ref,
    extra_ref,
    stream_ref,
    head_ref,
    load_sem,
    maps,
    from_state,
    from_values,
    totals,
    pair,
    sib,
    chip,
    zin1,
    zin2,
    zin4,
    zout1,
    zout2,
    zout4,
    hin,
    hout,
    mixed,
    mixed_in,
    head_whole,
    residual,
    rows,
    gated,
    hidden,
    shard,
    whole,
    far_out,
    relayed,
    outgoing,
    incoming,
    send_sem,
    recv_sem,
    ring_send,
    sib_send,
    ring_recv,
    sib_recv,
):
    z, y, c = lax.axis_index("sp_0"), lax.axis_index("sp_1"), lax.axis_index("sp_2")
    x = lax.axis_index("tp")
    to_sibling = {"sp_2": 1 - c}
    to_right, to_left, to_far = ({"tp": lax.rem(x + d, 4)} for d in (1, 3, 2))
    for ref in (zin1, zin2, zin4):
        ref[...] = jnp.zeros_like(ref)
    loads = {}
    pairs = (
        ("shards", gate_shard, shard.at[pl.ds(0, 32)]),
        ("shards", down_shard, shard.at[pl.ds(32, 32)]),
        ("shards", up_shard, shard.at[pl.ds(64, 32)]),
        ("local", strength_hbm, strength_ref),
        ("local", decay_hbm, decay_ref),
        ("local", extra_hbm, extra_ref),
        ("local", k_hbm, k_ref),
        ("local", q_hbm, q_ref),
        ("local", v_hbm, v_ref),
        ("shards", head_hbm, head_ref),
        ("late", gate_hbm, gate_ref),
        ("late", stream_hbm, stream_ref),
    )

    def arrived_loads(group):
        for load in loads[group]:
            load.wait()

    barrier = pltpu.get_barrier_semaphore()
    peers = [to_sibling, to_right, to_left, to_far]
    peers += [{"sp_1": lax.rem(y + d, 4)} for d in (1, 2, 3)]
    peers += [{"sp_0": lax.rem(z + d, 8)} for d in (1, 2, 4, 6, 7)]
    for peer in peers:
        pl.semaphore_signal(barrier, inc=1, device_id=peer, device_id_type=MESH)
    for n, (group, src, dst) in enumerate(pairs):
        load = pltpu.make_async_copy(src, dst, load_sem.at[n])
        load.start()
        loads.setdefault(group, []).append(load)

    gather = Gather(z, y, c, shard, whole, (ring_send, sib_send, ring_recv, sib_recv))
    schedule = iter(SCHEDULE)

    def pump():
        for event in next(schedule):
            gather.handle(*event)

    slots = iter(range(64))

    def copy(src, dst, peer):
        slot = next(slots)
        return pltpu.make_async_remote_copy(
            src_ref=src,
            dst_ref=dst,
            send_sem=send_sem.at[slot],
            recv_sem=recv_sem.at[slot],
            device_id=peer,
            device_id_type=MESH,
        )

    half = head_ref.at[pl.ds(pl.multiple_of(c * HEAD, HEAD), HEAD)]
    head_near = [
        copy(half, head_whole.at[LEFT, c], to_right),
        copy(half, head_whole.at[RIGHT, c], to_left),
    ]
    low, high = pl.ds(0, HEAD // 2), pl.ds(HEAD // 2, HEAD // 2)
    head_far = [
        copy(head_whole.at[LEFT, c, low], head_whole.at[FAR, c, low], to_right),
        copy(head_whole.at[RIGHT, c, high], head_whole.at[FAR, c, high], to_left),
    ]
    head_sib = [
        copy(head_whole.at[side, c], head_whole.at[side, c], to_sibling) for side in (FAR, RIGHT, LEFT)
    ]

    def begin():
        arrived_loads("shards")
        pl.semaphore_wait(barrier, len(peers))
        gather.start()
        for move in head_near:
            move.start()

    arrived_loads("local")
    local_part(
        q_ref,
        k_ref,
        v_ref,
        strength_ref,
        decay_ref,
        extra_ref,
        rate_ref,
        maps,
        from_state,
        from_values,
        begin,
        pump,
    )
    for h in range(2):
        total = joined(joined(maps[h], maps[2 + h]), maps[4 + h])
        totals[h] = total
        pair[h] = total.astype(BF16)

    to_sib = copy(pair.at[1 - c], sib, to_sibling)
    to_sib.start()
    pump()
    to_sib.wait()
    own, other = totals[c], sib[...].astype(F32)
    first = jnp.where(c == 0, own, other)
    chip[y] = joined(first, jnp.where(c == 0, other, own)).astype(BF16)
    totals[1] = first

    sends = []
    for d in (1, 2, 3):
        sends.append(copy(chip.at[y], chip.at[y], {"sp_1": lax.rem(y + d, 4)}))
        sends[-1].start()
    pump()
    for d in (1, 2, 3):
        sends[d - 1].wait()
    total = chip[0].astype(F32)
    before = jnp.where(y == 0, 0.0, total)
    for s in (1, 2, 3):
        total = joined(total, chip[s].astype(F32))
        if s < 3:
            before = jnp.where(y > s, total, before)

    totals[0] = before
    earlier = jnp.zeros((HEAD, 2 * HEAD), F32)
    for n, (d, out, arrived) in enumerate(((1, zout1, zin1), (2, zout2, zin2), (4, zout4, zin4))):
        out[...] = total[:, (2 * HEAD - out.shape[1]) :].astype(BF16)
        hop = copy(out, arrived, {"sp_0": lax.rem(z + d, 8)})

        @pl.when(z + d < 8)
        def _():
            hop.start()

        pump()

        @pl.when(z >= d)
        def _():
            hop.wait_recv()

        came = arrived[...].astype(F32)
        if d < 4:
            earlier = joined(came, earlier)
            total = joined(came, total)
        else:
            state = carried(came, earlier)

        @pl.when(z + d < 8)
        def _():
            hop.wait_send()

        if n == 0:
            for near, far in zip(head_near, head_far):
                near.wait_recv()
                far.start()
            head_sib[2].start()
            head_sib[1].start()
        if n == 2:
            for far in head_far:
                far.wait_recv()
            head_sib[0].start()

    arrived_loads("late")
    state = carried(state, totals[0])
    later = carried(state, totals[1])
    hout[...] = jnp.where(c == 0, later, state).astype(BF16)
    across = copy(hout, hin, to_sibling)
    across.start()

    def outputs(h, state):
        cols = pl.ds(pl.multiple_of(h * HEAD, HEAD), HEAD)
        for n in range(3):
            u = n * 2 + h
            span = slice(n * CHUNK, (n + 1) * CHUNK)
            out = from_values[u] + mm(from_state[u], state)
            if n < 2:
                state = carried(state, maps[u])
            out = out * lax.rsqrt(jnp.mean(out * out, axis=1, keepdims=True) + EPSILON)
            gated = out * gain_ref[...] * silu(gate_ref[span, cols].astype(F32))
            mixed[span, cols] = gated.astype(BF16)

    outputs(c, jnp.where(c == 0, state, later))
    pump()
    across.wait()
    outputs(1 - c, hin[...].astype(F32))

    def rows_of(d):
        return pl.ds(pl.multiple_of(lax.rem(x + d, 4) * TOK, TOK), TOK)

    exchange = [
        copy(mixed.at[rows_of(2)], mixed_in.at[FAR], to_far),
        copy(mixed.at[rows_of(1)], mixed_in.at[LEFT], to_right),
        copy(mixed.at[rows_of(3)], mixed_in.at[RIGHT], to_left),
    ]
    for move in exchange:
        move.start()
    pump()
    mixed_in[OWN] = mixed[rows_of(0), :]
    for move in head_sib:
        move.wait()
    head_whole[OWN] = head_ref[...].reshape(2, HEAD, -1)
    for move in exchange:
        move.wait()

    width = residual.shape[1]
    block = jnp.concatenate([mixed_in[side] for side in range(4)], axis=1)
    squares = jnp.zeros((TOK, 1), F32)
    for first in range(0, width, 2 * WIDE):
        cols = slice(first, first + 2 * WIDE)
        matrix = head_whole[:, :, :, cols].reshape(8 * HEAD, 2 * WIDE)
        tile = jnp.dot(block, matrix, preferred_element_type=F32) + stream_ref[:, cols].astype(F32)
        residual[:, cols] = tile
        squares = squares + jnp.sum(tile * tile, axis=1, keepdims=True)
    pump()
    scale = lax.rsqrt(squares / width + EPSILON)
    rows[OWN] = (residual[...] * scale * feed_gain_ref[...]).astype(BF16)

    top, bottom = pl.ds(0, TOK // 2), pl.ds(TOK // 2, TOK // 2)
    near = [
        copy(rows.at[OWN, top], rows.at[LEFT, top], to_right),
        copy(rows.at[OWN, bottom], rows.at[RIGHT, bottom], to_left),
        copy(rows.at[OWN, bottom], rows.at[LEFT, bottom], to_right),
        copy(rows.at[OWN, top], rows.at[RIGHT, top], to_left),
    ]
    for move in near:
        move.start()
    relay = [
        copy(rows.at[LEFT, top], rows.at[FAR, top], to_right),
        copy(rows.at[RIGHT, bottom], rows.at[FAR, bottom], to_left),
    ]
    pump()
    for move, onward in zip(near, relay):
        move.wait_recv()
        onward.start()
    pump()
    gather.from_sibling(0)

    units = hidden.shape[1]
    tiles = [slice(n, min(n + WIDE, units)) for n in range(0, units, WIDE)]

    def times(first, count, part, cols):
        matrix = whole[:, :, 32 * part : 32 * part + 32, cols].reshape(width, cols.stop - cols.start)
        block = rows[first : first + count].reshape(count * TOK, width)
        return jnp.dot(block, matrix, preferred_element_type=F32)

    near[2].wait_recv()
    near[3].wait_recv()
    for cols in tiles:
        gated[:, cols] = silu(times(RIGHT, 3, 0, cols))
        pump()
    pump()
    gather.from_sibling(2)
    for cols in tiles:
        hidden[TOK:, cols] = (gated[:, cols] * times(RIGHT, 3, 2, cols)).astype(BF16)
        pump()
    for move in relay:
        move.wait()
    for cols in tiles:
        far_gate = silu(times(FAR, 1, 0, cols))
        hidden[:TOK, cols] = (far_gate * times(FAR, 1, 2, cols)).astype(BF16)
    pump()
    gather.from_sibling(1)

    def down(first, count, store, part=(0, 2)):
        def step(n, carry):
            cols = pl.ds(pl.multiple_of(n * WIDE, WIDE), WIDE)
            matrix = whole[pl.ds(n * 4, 4), :, 32:64, :].reshape(WIDE, units)
            store(cols, mm_nt(hidden[first * TOK : (first + count) * TOK], matrix))
            return carry

        steps = width // WIDE // 2
        lax.fori_loop(part[0] * steps, part[1] * steps, step, 0)

    def store_far(cols, tile):
        far_out[:, cols] = tile.astype(BF16)

    def store_near(cols, tile):
        outgoing[:, :, cols] = tile.astype(BF16).reshape(2, TOK, WIDE)

    def store_own(cols, tile):
        residual[:, cols] = residual[:, cols] + tile

    far, direct, combined = [], [], []
    for part in range(2):
        cols = pl.ds(part * width // 2, width // 2)
        down(FAR, 1, store_far, (part, part + 1))
        far += [
            copy(far_out.at[top, cols], relayed.at[0, :, cols], to_right),
            copy(far_out.at[bottom, cols], relayed.at[1, :, cols], to_left),
        ]
        for move in far[-2:]:
            move.start()
    for part in range(2):
        cols = pl.ds(part * width // 2, width // 2)
        down(RIGHT, 2, store_near, (part, part + 1))
        direct += [
            copy(outgoing.at[0, bottom, cols], incoming.at[0, bottom, cols], to_right),
            copy(outgoing.at[1, top, cols], incoming.at[1, top, cols], to_left),
        ]
        for move in direct[-2:]:
            move.start()
    for part in range(2):
        cols = pl.ds(part * width // 2, width // 2)
        for side, rows_half in ((0, top), (1, bottom)):
            far[2 * part + side].wait_recv()
            mine = outgoing[side, rows_half, cols].astype(F32)
            outgoing[side, rows_half, cols] = (mine + relayed[side, :, cols].astype(F32)).astype(BF16)
        combined += [
            copy(outgoing.at[0, top, cols], incoming.at[0, top, cols], to_right),
            copy(outgoing.at[1, bottom, cols], incoming.at[1, bottom, cols], to_left),
        ]
        for move in combined[-2:]:
            move.start()
    down(OWN, 1, store_own)
    for move in direct + combined:
        move.wait()
    for move in far:
        move.wait_send()
    result_ref[...] = (
        residual[...] + (incoming[0].astype(F32) + incoming[1].astype(F32))
    ).astype(BF16)
    for move in near + head_near + head_far:
        move.wait_send()
    gather.finish()


SCHEDULE = (
    (("ds", 0),),
    (),
    (),
    (),
    (),
    (),
    (("uy", 1), ("gz", 1), ("gs", 1), ("gy", 0, 1), ("uz", 0, 1), ("us", 1),),
    (("gz", 2), ("gs", 2), ("uy", 2), ("dy", 0, 1), ("us", 2),),
    (("gz", 3), ("gs", 3), ("gy", 0, 2), ("gy", 1, 1), ("us", 3), ("dz", 1),),
    (("uz", 0, 2), ("uz", 1, 1), ("uz", 2, 1), ("gz", 4), ("gs", 4), ("dy", 0, 2), ("ds", 1), ("gy", 2, 1),),
    (("uz", 3, 1), ("dz", 2), ("gy", 3, 1),),
    (("gy", 1, 2), ("ds", 2),),
    (("uz", 3, 2), ("uz", 0, 3), ("uz", 1, 2), ("uz", 2, 2), ("gy", 4, 1),),
    (("gy", 2, 2), ("gy", 3, 2), ("dy", 1, 1), ("dz", 3), ("ds", 3),),
    (("uz", 0, 4), ("uz", 1, 3), ("uz", 3, 3), ("uz", 2, 3), ("gy", 4, 2), ("dy", 2, 1), ("dz", 4), ("ds", 4),),
    (("dy", 3, 1),),
    (),
    (),
    (),
    (),
    (),
    (("uz", 1, 4), ("uz", 2, 4), ("uz", 3, 4),),
    (("dy", 1, 2), ("dy", 4, 1),),
    (),
    (),
    (("dy", 2, 2),),
    (),
    (("dy", 3, 2),),
    (("dy", 4, 2),),
)


def body(
    stream,
    query_projected,
    key_projected,
    value_projected,
    gate_projected,
    strength_logits,
    decay_preactivation,
    extra_log_decay,
    head_decay_rate,
    head_norm_gain,
    head_output_matrix,
    feed_norm_gain,
    gate_matrix,
    up_matrix,
    down_matrix,
):
    width = stream.shape[1]
    units = gate_matrix.shape[1]
    vmem = pl.BlockSpec(memory_space=pltpu.VMEM)
    hbm = pl.BlockSpec(memory_space=pl.ANY)
    tokens = query_projected.shape[0]
    pair = (HEAD, 2 * HEAD)
    square = (HEAD, HEAD)
    return pl.pallas_call(
        layer_kernel,
        name="layer",
        out_shape=jax.ShapeDtypeStruct(stream.shape, BF16),
        in_specs=[hbm] * 7 + [pl.BlockSpec(memory_space=pltpu.SMEM), vmem] + [hbm] * 2 + [vmem] + [hbm] * 3,
        out_specs=vmem,
        scratch_shapes=[
            *[pltpu.VMEM((tokens, 2 * HEAD), BF16)] * 4,
            pltpu.VMEM((2, tokens), BF16),
            pltpu.VMEM((2, tokens), BF16),
            pltpu.VMEM((2, tokens), F32),
            pltpu.VMEM((TOK, width), BF16),
            pltpu.VMEM((2 * HEAD, width), BF16),
            pltpu.SemaphoreType.DMA((12,)),
            pltpu.VMEM((6, *pair), F32),
            pltpu.VMEM((6, *square), BF16),
            pltpu.VMEM((6, *square), F32),
            pltpu.VMEM((2, *pair), F32),
            pltpu.VMEM((2, *pair), BF16),
            pltpu.VMEM(pair, BF16),
            pltpu.VMEM((4, *pair), BF16),
            pltpu.VMEM(pair, BF16),
            pltpu.VMEM(pair, BF16),
            pltpu.VMEM(square, BF16),
            pltpu.VMEM(pair, BF16),
            pltpu.VMEM(pair, BF16),
            pltpu.VMEM(square, BF16),
            pltpu.VMEM(square, BF16),
            pltpu.VMEM(square, BF16),
            pltpu.VMEM((4 * TOK, 2 * HEAD), BF16),
            pltpu.VMEM((4, TOK, 2 * HEAD), BF16),
            pltpu.VMEM((4, 2, HEAD, width), BF16),
            pltpu.VMEM((TOK, width), F32),
            pltpu.VMEM((4, TOK, width), BF16),
            pltpu.VMEM((3 * TOK, units), F32),
            pltpu.VMEM((4 * TOK, units), BF16),
            pltpu.VMEM((96, units), BF16),
            pltpu.VMEM((32, 2, 96, units), BF16),
            pltpu.VMEM((TOK, width), BF16),
            pltpu.VMEM((2, TOK // 2, width), BF16),
            pltpu.VMEM((2, TOK, width), BF16),
            pltpu.VMEM((2, TOK, width), BF16),
            pltpu.SemaphoreType.DMA((48,)),
            pltpu.SemaphoreType.DMA((48,)),
            pltpu.SemaphoreType.DMA,
            pltpu.SemaphoreType.DMA,
            pltpu.SemaphoreType.DMA((144,)),
            pltpu.SemaphoreType.DMA((3,)),
        ],
        compiler_params=pltpu.CompilerParams(
            collective_id=0, has_side_effects=True, vmem_limit_bytes=60 * 1024 * 1024
        ),
    )(
        query_projected,
        key_projected,
        value_projected,
        gate_projected,
        strength_logits,
        decay_preactivation,
        extra_log_decay,
        head_decay_rate,
        head_norm_gain[None, :],
        stream,
        head_output_matrix,
        feed_norm_gain[None, :],
        gate_matrix,
        up_matrix,
        down_matrix.T,
    )


def solution(mesh):
    torus = Mesh(mesh.devices.reshape(8, 4, 2, mesh.shape["tp"]), ("sp_0", "sp_1", "sp_2", "tp"))
    in_specs = (
        P(SP_TP, None),
        P(SP, "tp"),
        P(SP, "tp"),
        P(SP, "tp"),
        P(SP, "tp"),
        P("tp", SP),
        P("tp", SP),
        P("tp", SP),
        P("tp"),
        P(),
        P("tp", None),
        P(),
        P(SP, "tp"),
        P(SP, "tp"),
        P("tp", SP),
    )
    out_specs = P(SP_TP, None)
    return jax.shard_map(body, mesh=torus, in_specs=in_specs, out_specs=out_specs, check_vma=False)
```
